32 devices in a mesh: fs: 8 (over z, y), tp: 4 (over x, core).
Axes of the slice: x: 2, y: 2, z: 4, core: 2. Of those that a mesh axis runs over, the one named last changes fastest.
Arguments:
- saved_input: bfloat16 [6144, 2048], P('fs'), may hold values from -6 to 6
- cot_inproj: bfloat16 [6144, 1024], P('fs', 'tp'), may hold values from -0.076171875 to 0.076171875
- cot_outproj: bfloat16 [6144, 1024], P('fs', 'tp'), may hold values from -0.076171875 to 0.076171875
- factor_inproj: bfloat16 [2048, 256], P('fs')
- factor_outproj: bfloat16 [2048, 256], P('fs')
- weight_inproj: float32 [2048, 1024], P('fs', 'tp'), may hold values from -0.125 to 0.125
- weight_outproj: float32 [2048, 1024], P('fs', 'tp'), may hold values from -0.125 to 0.125
- first_inproj: float32 [256, 1024], P('fs', 'tp'), may hold values from -6 to 6
- first_outproj: float32 [256, 1024], P('fs', 'tp'), may hold values from -6 to 6
- second_inproj: float32 [256, 1024], P('fs', 'tp'), may hold values from 0.25 to 4
- second_outproj: float32 [256, 1024], P('fs', 'tp'), may hold values from 0.25 to 4
Outputs:
- update_inproj: float32 [2048, 1024], P('fs', 'tp')
- update_outproj: float32 [2048, 1024], P('fs', 'tp')
- new_inproj: float32 [2048, 1024], P('fs', 'tp')
- new_outproj: float32 [2048, 1024], P('fs', 'tp')
- copy_inproj: bfloat16 [2048, 1024], P(None, 'tp')
- copy_outproj: bfloat16 [2048, 1024], P(None, 'tp')
- first_inproj_new: float32 [256, 1024], P('fs', 'tp')
- first_outproj_new: float32 [256, 1024], P('fs', 'tp')
- second_inproj_new: float32 [256, 1024], P('fs', 'tp')
- second_outproj_new: float32 [256, 1024], P('fs', 'tp')
The draws below stay inside these ranges and needn't reach their ends.
All inputs are finite; a program needn't handle non-finite values.
Results may differ from the reference program's by a relative error of at most 0.00045.
Values may be sent and summed in bfloat16 or wider, within the bound.
A program may use at most 64 MiB of HBM per device.

```python
import math
import jax
import jax.numpy as jnp
from jax import lax

D = 2048
RANK = 256
GN = 1024
TOKENS = 6144


def lowrank_draw(key):
    base = jax.random.normal(key, (D, RANK), jnp.float32)
    position = jnp.arange(D).astype(jnp.float32) / D
    scale = jnp.exp(jnp.log(10.0) * position) * 0.22 * D ** (-0.5)
    return (base * scale[:, None]).astype(jnp.bfloat16)


def draw_factor_inproj(key, part):
    return lowrank_draw(jax.random.fold_in(key, 11))


def draw_factor_outproj(key, part):
    return lowrank_draw(jax.random.fold_in(key, 12))


def raised(values, stream_key, source, target, shards_of, factor):
    owner, partner = [(jnp.arange(values.shape[dim]) // (values.shape[dim] // shards_of)).reshape([-1 if axis == dim else 1 for axis in range(values.ndim)]) for dim in (source, target)]
    chosen = jax.random.permutation(stream_key, shards_of)[partner]
    strong = (owner == chosen) | (owner == (partner + shards_of // 2) % shards_of)
    return jnp.where(strong, factor * values, values)


def levels(rng, shape, cuts, least, high):
    level = 1.0
    for axis_at, shards_of in cuts:
        draws = jax.random.uniform(jax.random.fold_in(jax.random.fold_in(rng, 6), axis_at), (shards_of,), jnp.float32, least / len(cuts), high / len(cuts))
        level = level * jnp.repeat(jnp.exp(draws), shape[axis_at] // shards_of).reshape((-1,) + (1,) * (len(shape) - 1 - axis_at))
    return level


def normal_values(key, dims, spread, most, cuts=(), kind=jnp.bfloat16):
    array = spread * jax.random.normal(key, dims, jnp.float32)
    if cuts:
        array = array * levels(key, dims, cuts, -0.22, 0.18)
    return jnp.clip(array, -most, most).astype(kind)


def gaussian_with(stream_key, shape, width, limit, split, heavy, kind=jnp.bfloat16):
    array = width * jax.random.normal(stream_key, shape, jnp.float32)
    if split:
        array = array * levels(stream_key, shape, split, -0.22, 0.18)
    return jnp.clip(raised(array, jax.random.fold_in(stream_key, 3), *heavy), -limit, limit).astype(kind)


def setup_inputs(seed: int = 0) -> dict:
    streams_of = jax.random.split(jax.random.key(seed), 12)
    saved_input = gaussian_with(streams_of[0], (TOKENS, D), 1.0, 6.0, ((0, 8),), (0, 1, 8, 2.0))
    cot_inproj = normal_values(streams_of[1], (TOKENS, GN), (TOKENS ** -0.5), 0.076171875, ((0, 8), (1, 4)))
    cot_outproj = normal_values(streams_of[2], (TOKENS, GN), (TOKENS ** -0.5), 0.076171875, ((0, 8), (1, 4)))
    factor_inproj = draw_factor_inproj(jax.random.fold_in(streams_of[11], 71), 0)
    factor_outproj = draw_factor_outproj(jax.random.fold_in(streams_of[11], 71), 0)
    weight_inproj = normal_values(streams_of[5], (D, GN), D ** -0.5, 0.125, ((0, 8), (1, 4)), jnp.float32)
    weight_outproj = normal_values(streams_of[6], (D, GN), D ** -0.5, 0.125, ((0, 8), (1, 4)), jnp.float32)
    first_inproj = normal_values(streams_of[7], (RANK, GN), 1.0, 6.0, ((0, 8), (1, 4)), jnp.float32)
    first_outproj = normal_values(streams_of[8], (RANK, GN), 1.0, 6.0, ((0, 8), (1, 4)), jnp.float32)
    second_inproj = jnp.clip(jnp.exp(math.log(4.0) - 2.7725887 * jax.random.uniform(streams_of[9], (RANK, GN), jnp.float32) ** levels(streams_of[9], (RANK, GN), ((0, 8), (1, 4)), -0.2, 0.2)), 0.25, 4.0)
    second_outproj = jnp.clip(jnp.exp(math.log(4.0) - 2.7725887 * jax.random.uniform(streams_of[10], (RANK, GN), jnp.float32) ** levels(streams_of[10], (RANK, GN), ((0, 8), (1, 4)), -0.2, 0.2)), 0.25, 4.0)
    return dict(saved_input=saved_input, cot_inproj=cot_inproj, cot_outproj=cot_outproj, factor_inproj=factor_inproj, factor_outproj=factor_outproj, weight_inproj=weight_inproj, weight_outproj=weight_outproj, first_inproj=first_inproj, first_outproj=first_outproj, second_inproj=second_inproj, second_outproj=second_outproj)


def one_matrix(saved_input, cotangent, factor, weight, first, second):
    grad = lax.dot_general(saved_input, cotangent, (((0,), (0,)), ((), ())), preferred_element_type=jnp.float32)
    factor_wide = factor.astype(jnp.float32)
    projected = lax.dot_general(factor_wide, grad, (((0,), (0,)), ((), ())), precision=lax.Precision.HIGHEST)
    first_new = 0.8 * first + 0.2 * projected
    second_new = 0.9 * second + 0.1 * projected * projected
    small = first_new / (jnp.sqrt(second_new) + 1e-08)
    full = jnp.dot(factor_wide, small, precision=lax.Precision.HIGHEST)
    update = full / jnp.sqrt(jnp.mean(full * full) + 1e-06)
    fresh = weight - 0.02 * update
    return (update, fresh, fresh.astype(jnp.bfloat16), first_new, second_new)

def reference(saved_input, cot_inproj, cot_outproj, factor_inproj, factor_outproj, weight_inproj, weight_outproj, first_inproj, first_outproj, second_inproj, second_outproj):
    in_parts = one_matrix(saved_input, cot_inproj, factor_inproj, weight_inproj, first_inproj, second_inproj)
    out_parts = one_matrix(saved_input, cot_outproj, factor_outproj, weight_outproj, first_outproj, second_outproj)
    return (in_parts[0], out_parts[0], in_parts[1], out_parts[1], in_parts[2], out_parts[2], in_parts[3], out_parts[3], in_parts[4], out_parts[4])
```

```python
import functools

import jax
import jax.numpy as jnp
from jax import lax
from jax.experimental import pallas as pl
from jax.experimental.pallas import tpu as pltpu
from jax.sharding import PartitionSpec as P


def contract_rows(left, right, precision):
    return lax.dot_general(
        left,
        right,
        (((0,), (0,)), ((), ())),
        precision=precision,
        preferred_element_type=jnp.float32,
    )


def plain_form(
    saved_input,
    cot_inproj,
    cot_outproj,
    factor_inproj,
    factor_outproj,
    weight_inproj,
    weight_outproj,
    first_inproj,
    first_outproj,
    second_inproj,
    second_outproj,
):
    highest = lax.Precision.HIGHEST
    pieces = (
        lax.all_gather(factor_inproj, "fs", axis=0, tiled=True),
        lax.all_gather(factor_outproj, "fs", axis=0, tiled=True),
    )
    mapped_in = jnp.dot(saved_input, pieces[0], preferred_element_type=jnp.float32)
    mapped_out = jnp.dot(saved_input, pieces[1], preferred_element_type=jnp.float32)
    term_in = contract_rows(mapped_in, cot_inproj.astype(jnp.float32), highest)
    term_out = contract_rows(mapped_out, cot_outproj.astype(jnp.float32), highest)
    projected_in, projected_out = (
        lax.psum_scatter(term_in, "fs", scatter_dimension=0, tiled=True),
        lax.psum_scatter(term_out, "fs", scatter_dimension=0, tiled=True),
    )
    first_in_new = 0.8 * first_inproj + 0.2 * projected_in
    first_out_new = 0.8 * first_outproj + 0.2 * projected_out
    second_in_new = 0.9 * second_inproj + 0.1 * projected_in * projected_in
    second_out_new = 0.9 * second_outproj + 0.1 * projected_out * projected_out
    small_in = first_in_new / (jnp.sqrt(second_in_new) + 1e-08)
    small_out = first_out_new / (jnp.sqrt(second_out_new) + 1e-08)
    wide_in = factor_inproj.astype(jnp.float32)
    wide_out = factor_outproj.astype(jnp.float32)
    pieces = (
        lax.all_gather(small_in, "fs", axis=0, tiled=True),
        lax.all_gather(small_out, "fs", axis=0, tiled=True),
    )
    full_in = jnp.dot(wide_in, pieces[0], precision=highest)
    full_out = jnp.dot(wide_out, pieces[1], precision=highest)
    square_in, square_out = lax.psum(
        (jnp.sum(full_in * full_in), jnp.sum(full_out * full_out)), ("fs", "tp")
    )
    entries = float(full_in.shape[0] * full_in.shape[1] * lax.axis_size("fs") * lax.axis_size("tp"))
    update_in = full_in / jnp.sqrt(square_in / entries + 1e-06)
    update_out = full_out / jnp.sqrt(square_out / entries + 1e-06)
    fresh_in = weight_inproj - 0.02 * update_in
    fresh_out = weight_outproj - 0.02 * update_out
    copy_in, copy_out = (
        lax.all_gather(fresh_in.astype(jnp.bfloat16), "fs", axis=0, tiled=True),
        lax.all_gather(fresh_out.astype(jnp.bfloat16), "fs", axis=0, tiled=True),
    )
    return (
        update_in,
        update_out,
        fresh_in,
        fresh_out,
        copy_in,
        copy_out,
        first_in_new,
        first_out_new,
        second_in_new,
        second_out_new,
    )


MESH = pl.DeviceIdType.MESH
F32, BF16 = jnp.float32, jnp.bfloat16


def parts_of(x):
    high = x.astype(BF16)
    return high, (x - high.astype(F32)).astype(BF16)


def dot(a, b):
    return jnp.dot(a, b, preferred_element_type=F32)


class Gather:
    def goes_up(self, s):
        z, last = self.z, self.depth - 1
        needed = (z - s >= 0) & (z < last)
        return needed & (z != last - 1) if self.near and s == 0 else needed

    def goes_down(self, s):
        z, last = self.z, self.depth - 1
        needed = (z + s <= last) & (z >= 1)
        return needed & (z != 1) if self.near and s == 0 else needed

    def crosses(self, zi, c):
        sent = jnp.logical_not(self.detour(zi, c))
        return sent & (zi != self.z) if self.near else sent

    def __init__(self, place, chunks, ref_of, sems, near=False):
        self.z, self.y, self.tp, self.depth = place
        self.near = near
        self.chunks, self.ref_of = chunks, ref_of
        self.up_s, self.up_r, self.dn_s, self.dn_r, self.y_s, self.y_r, self.x_s, self.x_r = sems

    def detour(self, zi, c):
        z, last = self.z, self.depth - 1
        if self.depth < 4:
            return z < 0
        end = ((z == 1) & (zi == 0)) | ((z == last - 1) & (zi == last))
        if c >= self.chunks // 2:
            end = end | ((z == 0) & (zi == 1)) | ((z == last) & (zi == last - 1))
        return end

    def copy(self, zi, yi, c, s_sem, r_sem, to_z, to_y):
        ref = self.ref_of(zi * 2 + yi, c)
        return pltpu.make_async_remote_copy(
            src_ref=ref, dst_ref=ref, send_sem=s_sem, recv_sem=r_sem,
            device_id=(to_z * 2 + to_y, self.tp), device_id_type=MESH,
        )

    def up(self, s, c):
        return self.copy(self.z - s, self.y, c, self.up_s.at[s, c], self.up_r.at[s, c], self.z + 1, self.y)

    def down(self, s, c):
        return self.copy(self.z + s, self.y, c, self.dn_s.at[s, c], self.dn_r.at[s, c], self.z - 1, self.y)

    def from_below(self, s, c):
        return self.copy(self.z - 1 - s, self.y, c, self.up_s.at[s, c], self.up_r.at[s, c], self.z, self.y)

    def from_above(self, s, c):
        return self.copy(self.z + 1 + s, self.y, c, self.dn_s.at[s, c], self.dn_r.at[s, c], self.z, self.y)

    def across(self, zi, c):
        return self.copy(zi, self.y, c, self.y_s.at[zi, c], self.y_r.at[zi, c], self.z, 1 - self.y)

    def from_across(self, zi, c):
        return self.copy(zi, 1 - self.y, c, self.y_s.at[zi, c], self.y_r.at[zi, c], self.z, self.y)

    def beside(self, c, to_z):
        return self.copy(self.z, 1 - self.y, c, self.x_s.at[c], self.x_r.at[c], to_z, self.y)

    def from_beside(self, zi, c):
        return self.copy(zi, 1 - self.y, c, self.x_s.at[c], self.x_r.at[c], self.z, self.y)

    def beside_cases(self, c):
        if self.depth < 4:
            return ()
        z, last = self.z, self.depth - 1
        cases = [(z == 0, 1), (z == last, last - 1)]
        if c >= self.chunks // 2:
            cases += [(z == 1, 0), (z == last - 1, last)]
        return cases

    def start(self, c):
        @pl.when(self.goes_up(0))
        def _():
            self.up(0, c).start()

        @pl.when(self.goes_down(0))
        def _():
            self.down(0, c).start()

        if not self.near:
            self.across(self.z, c).start()

    def start_beside(self, c):
        for condition, neighbour in self.beside_cases(c):
            @pl.when(condition)
            def _():
                self.beside(c, neighbour).start()

    def hand_on(self, zi, c):
        @pl.when(jnp.logical_not(self.detour(zi, c)))
        def _():
            self.across(zi, c).start()

    def land(self, zi, c, have):
        gone = self.detour(zi, c)

        @pl.when(gone)
        def _():
            self.from_beside(zi, c).wait_recv()

        @pl.when(jnp.logical_not(gone))
        def _():
            self.from_across(zi, c).wait_recv()

        have(zi * 2 + 1 - self.y, c)

    def relay(self, have=None, after=None):
        have = have or (lambda block, c: None)
        z, depth = self.z, self.depth
        for s in range(1, depth + 1):
            for c in range(self.chunks):
                if s < depth:
                    @pl.when(z - s >= 0)
                    def _():
                        if self.near and s == 1:
                            @pl.when(z != depth - 1)
                            def _():
                                self.from_below(0, c).wait_recv()
                        else:
                            self.from_below(s - 1, c).wait_recv()
                        if s < depth - 1:
                            @pl.when(z + 1 < depth)
                            def _():
                                self.up(s, c).start()
                        self.hand_on(z - s, c)
                        have((z - s) * 2 + self.y, c)

                    @pl.when(z + s < depth)
                    def _():
                        if self.near and s == 1:
                            @pl.when(z != 0)
                            def _():
                                self.from_above(0, c).wait_recv()
                        else:
                            self.from_above(s - 1, c).wait_recv()
                        if s < depth - 1:
                            @pl.when(z >= 1)
                            def _():
                                self.down(s, c).start()
                        self.hand_on(z + s, c)
                        have((z + s) * 2 + self.y, c)

                if s == 1:
                    if not self.near:
                        self.from_across(z, c).wait_recv()
                        self.start_beside(c)
                        have(z * 2 + 1 - self.y, c)
                else:
                    @pl.when(z - (s - 1) >= 0)
                    def _():
                        self.land(z - (s - 1), c, have)

                    @pl.when(z + (s - 1) < depth)
                    def _():
                        self.land(z + (s - 1), c, have)
            if after is not None:
                after(s)

    def finish(self):
        for c in range(self.chunks):
            for s in range(self.depth - 1):
                @pl.when(self.goes_up(s))
                def _():
                    self.up(s, c).wait_send()

                @pl.when(self.goes_down(s))
                def _():
                    self.down(s, c).wait_send()
            for zi in range(self.depth):
                @pl.when(self.crosses(zi, c))
                def _():
                    self.across(zi, c).wait_send()
            for condition, neighbour in self.beside_cases(c):
                @pl.when(condition)
                def _():
                    self.beside(c, neighbour).wait_send()


class Late:
    def __init__(self, place, chunks, ref_of, sems):
        self.z, self.y, self.tp, self.depth = place
        self.chunks, self.ref_of = chunks, ref_of
        self.up_s, self.up_r, self.dn_s, self.dn_r, self.y_s, self.y_r, self.x_s, self.x_r = sems
        self.last = self.depth - 1
        self.at_end = (self.z == 0) | (self.z == self.last)
        self.far = self.last - self.z
        self.inner = jnp.where(self.z == 0, 1, self.last - 1)
        self.outer = jnp.where(self.z == 1, 0, self.last)

    def second(self, c):
        return c >= self.chunks // 2

    def copy(self, zi, yi, c, s_sem, r_sem, to_z, to_y):
        ref = self.ref_of(zi * 2 + yi, c)
        return pltpu.make_async_remote_copy(
            src_ref=ref, dst_ref=ref, send_sem=s_sem, recv_sem=r_sem,
            device_id=(to_z * 2 + to_y, self.tp), device_id_type=MESH,
        )

    def up(self, s, c):
        return self.copy(self.z - s, self.y, c, self.up_s.at[s, c], self.up_r.at[s, c], self.z + 1, self.y)

    def down(self, s, c):
        return self.copy(self.z + s, self.y, c, self.dn_s.at[s, c], self.dn_r.at[s, c], self.z - 1, self.y)

    def from_below(self, s, c):
        return self.copy(self.z - 1 - s, self.y, c, self.up_s.at[s, c], self.up_r.at[s, c], self.z, self.y)

    def from_above(self, s, c):
        return self.copy(self.z + 1 + s, self.y, c, self.dn_s.at[s, c], self.dn_r.at[s, c], self.z, self.y)

    def across(self, zi, c):
        return self.copy(zi, self.y, c, self.y_s.at[zi, c], self.y_r.at[zi, c], self.z, 1 - self.y)

    def from_across(self, zi, c):
        return self.copy(zi, 1 - self.y, c, self.y_s.at[zi, c], self.y_r.at[zi, c], self.z, self.y)

    def beside(self, zi, c, to_z):
        return self.copy(zi, 1 - self.y, c, self.x_s.at[c], self.x_r.at[c], to_z, self.y)

    def sidesteps(self, c):
        return c >= 1

    def crosses(self, zi, c):
        gap = jnp.abs(self.z - zi)
        near = jnp.where(self.at_end, True, zi != self.z)
        if self.sidesteps(c):
            near = near & jnp.logical_not(self.at_end & (gap == 1))
        if self.second(c):
            return near
        near = near & jnp.logical_not(jnp.logical_not(self.at_end) & (gap == 2))
        return near & (gap != self.last)

    def goes_up(self, s):
        return (self.z - s >= 0) & (self.z < self.last)

    def goes_down(self, s):
        return (self.z + s <= self.last) & (self.z >= 1)

    def start_own(self, c):
        @pl.when(self.goes_up(0))
        def _():
            self.up(0, c).start()

        @pl.when(self.goes_down(0))
        def _():
            self.down(0, c).start()

        @pl.when(self.at_end)
        def _():
            self.across(self.z, c).start()

    def start_far(self, c):
        if self.second(c):
            self.across(self.far, c).start()
        else:
            self.beside(self.far, c, self.inner).start()

    def start_beside(self, c):
        if self.sidesteps(c):
            self.beside(self.z, c, self.outer).start()

    def hand_on(self, zi, c):
        @pl.when(self.crosses(zi, c))
        def _():
            self.across(zi, c).start()

    def relay(self):
        z, depth = self.z, self.depth
        for s in range(1, depth - 1):
            for c in range(self.chunks):
                @pl.when(z - s >= 0)
                def _():
                    self.from_below(s - 1, c).wait_recv()
                    if s < depth - 2:
                        @pl.when(z + 1 < depth)
                        def _():
                            self.up(s, c).start()
                    self.hand_on(z - s, c)

                @pl.when(z + s < depth)
                def _():
                    self.from_above(s - 1, c).wait_recv()
                    if s < depth - 2:
                        @pl.when(z >= 1)
                        def _():
                            self.down(s, c).start()
                    self.hand_on(z + s, c)
        for c in range(self.chunks):
            for zi in range(depth):
                @pl.when(self.crosses(zi, c))
                def _():
                    self.from_across(zi, c).wait_recv()
            if not self.second(c):
                @pl.when(jnp.logical_not(self.at_end))
                def _():
                    self.from_beside(self.last - self.outer, c).wait_recv()
            if self.sidesteps(c):
                @pl.when(self.at_end)
                def _():
                    self.from_beside(self.inner, c).wait_recv()

    def from_beside(self, zi, c):
        return self.copy(zi, 1 - self.y, c, self.x_s.at[c], self.x_r.at[c], self.z, self.y)

    def finish(self):
        for c in range(self.chunks):
            for s in range(self.depth - 2):
                @pl.when(self.goes_up(s))
                def _():
                    self.up(s, c).wait_send()

                @pl.when(self.goes_down(s))
                def _():
                    self.down(s, c).wait_send()
            for zi in range(self.depth):
                @pl.when(self.crosses(zi, c))
                def _():
                    self.across(zi, c).wait_send()
            if not self.second(c):
                @pl.when(self.at_end)
                def _():
                    self.beside(self.far, c, self.inner).wait_send()
            if self.sidesteps(c):
                @pl.when(jnp.logical_not(self.at_end))
                def _():
                    self.beside(self.z, c, self.outer).wait_send()


def gather_sems(depth, chunks):
    dma = pltpu.SemaphoreType.DMA
    return [dma((depth - 1, chunks))] * 4 + [dma((depth, chunks))] * 2 + [dma((chunks,))] * 2


def kernel(
    n, tps, entries,
    saved_hbm, cot_in_hbm, cot_out_hbm, factor_in_hbm, factor_out_hbm, weight_in_hbm, weight_out_hbm,
    first_in_hbm, first_out_hbm, second_in_hbm, second_out_hbm,
    update, fresh, copies, first_new, second_new,
    saved, cots, factors, weights, first, second, mapped, terms, crossed, staged, landed, smalls, squares, early, ahead,
    wy_s, wy_r, wz_s, wz_r, load_sem, pair_s, pair_r, ty_s, ty_r, tz_s, tz_r, sz_s, sz_r, sy_s, sy_r, norm_s, norm_r, *gather_refs,
):
    me, tp = lax.axis_index("fs"), lax.axis_index("tp")
    z, y = me // 2, me % 2
    depth = n // 2
    side = tp % 2
    partner = tp + 1 - 2 * side
    rows = factors.shape[2]
    half = rows // 2
    slim = first.shape[1]
    place = (z, y, tp, depth)

    barrier = pltpu.get_barrier_semaphore()
    for k in range(1, depth):
        pl.semaphore_signal(barrier, inc=1, device_id=((z + k) % depth * 2 + y, tp), device_id_type=MESH)
    pl.semaphore_signal(barrier, inc=1, device_id=(z * 2 + 1 - y, tp), device_id_type=MESH)
    for k in range(1, tps):
        pl.semaphore_signal(barrier, inc=1, device_id=(me, (tp + k) % tps), device_id_type=MESH)

    loads = [
        pltpu.make_async_copy(source, target, load_sem.at[i])
        for i, (source, target) in enumerate((
            (factor_in_hbm, factors.at[0, me]), (factor_out_hbm, factors.at[1, me]),
            (saved_hbm, saved), (cot_in_hbm, cots.at[0]), (cot_out_hbm, cots.at[1]),
            (first_in_hbm, first.at[0]), (first_out_hbm, first.at[1]),
            (second_in_hbm, second.at[0]), (second_out_hbm, second.at[1]),
            (weight_in_hbm, weights.at[0]), (weight_out_hbm, weights.at[1]),
        ))
    ]
    for load in loads:
        load.start()
    loads[0].wait()
    loads[1].wait()
    pl.semaphore_wait(barrier, depth + tps - 1)

    def factor_ref(m, block, c):
        return factors.at[m, block, pl.ds(c * half, half)]

    def hand(m, block, c):
        ref = factor_ref(m, block, c)
        return pltpu.make_async_remote_copy(
            src_ref=ref, dst_ref=ref, send_sem=pair_s.at[block, c], recv_sem=pair_r.at[block, c],
            device_id=(me, partner), device_id_type=MESH,
        )

    gather = Gather(place, 2, lambda block, c: factor_ref(side, block, c), gather_refs[:8])
    gather.start(0)
    gather.start(1)
    loads[2].wait()

    def map_block(block, first_one=False):
        piece = saved[:, pl.ds(pl.multiple_of(block * rows, rows), rows)]
        for m in range(2):
            product = dot(piece, factors[m, block])
            mapped[m] = product if first_one else mapped[m] + product

    def map_handed(block):
        for c in range(2):
            hand(1 - side, block, c).wait_recv()
        map_block(block)

    def map_at(distance):
        if distance == 0:
            map_handed(z * 2 + 1 - y)
            return

        @pl.when(z - distance >= 0)
        def _():
            map_handed((z - distance) * 2 + y)
            map_handed((z - distance) * 2 + 1 - y)

        @pl.when(z + distance < depth)
        def _():
            map_handed((z + distance) * 2 + y)
            map_handed((z + distance) * 2 + 1 - y)

    at_end = (z == 0) | (z == depth - 1)
    middle = jnp.logical_not(at_end)
    far = depth - 1 - z

    def early_cross(m, c):
        part = pl.ds(c * half, half)
        return pltpu.make_async_remote_copy(
            src_ref=weights.at[m, part], dst_ref=early.at[0, m, part],
            send_sem=wy_s.at[m, c], recv_sem=wy_r.at[m, c], device_id=(z * 2 + 1 - y, tp), device_id_type=MESH,
        )

    def early_far(m, c):
        part = pl.ds(c * half, half)
        return pltpu.make_async_remote_copy(
            src_ref=weights.at[m, part], dst_ref=early.at[0, m, part],
            send_sem=wz_s.at[m, c], recv_sem=wz_r.at[m, c], device_id=(far * 2 + y, tp), device_id_type=MESH,
        )

    def far_cross(c):
        part = pl.ds(c * half, half)
        return pltpu.make_async_remote_copy(
            src_ref=early.at[0, 0, part], dst_ref=early.at[1, 0, part],
            send_sem=wy_s.at[0, c], recv_sem=wy_r.at[0, c], device_id=(z * 2 + 1 - y, tp), device_id_type=MESH,
        )

    def far_start(m):
        @pl.when(at_end)
        def _():
            for c in range(2):
                early_far(m, c).start()

    def far_cross_start(c):
        @pl.when(at_end)
        def _():
            early_far(0, c).wait_recv()
            far_cross(c).start()

    def cross_start(m, c):
        @pl.when(middle)
        def _():
            early_cross(m, c).start()

    def after_hop(s):
        if s >= 2:
            map_at(s - 2)
        if s == 2:
            loads[9].wait()
            loads[10].wait()
            far_start(0)

    map_block(me, True)
    gather.relay(
        lambda block, c: hand(side, block, c).start(),
        after_hop,
    )
    for load in loads[3:9]:
        load.wait()
    cross_start(0, 0)
    far_start(1)
    map_at(depth - 1)

    def term_cross(m, zi):
        return pltpu.make_async_remote_copy(
            src_ref=terms.at[m, zi * 2 + 1 - y], dst_ref=crossed.at[m, zi],
            send_sem=ty_s.at[m, zi], recv_sem=ty_r.at[m, zi],
            device_id=(z * 2 + 1 - y, tp), device_id_type=MESH,
        )

    def term_along(m, zi):
        return pltpu.make_async_remote_copy(
            src_ref=staged.at[m, zi], dst_ref=landed.at[m, z], send_sem=tz_s.at[m, zi], recv_sem=tz_r.at[m, z],
            device_id=(zi * 2 + y, tp), device_id_type=MESH,
        )

    def term_from(m, zi):
        return pltpu.make_async_remote_copy(
            src_ref=staged.at[m, z], dst_ref=landed.at[m, zi], send_sem=tz_s.at[m, z], recv_sem=tz_r.at[m, zi],
            device_id=(z * 2 + y, tp), device_id_type=MESH,
        )

    order = [k % depth for k in range(1, depth + 1)]
    for m in range(2):
        high, rest = parts_of(mapped[m].T)
        term = dot(high, cots[m]) + dot(rest, cots[m])
        terms[m] = term.reshape(n, slim, term.shape[1])
        for k in order:
            term_cross(m, (z + k) % depth).start()
    for m in range(2):
        for k in order:
            zi = (z + k) % depth
            term_cross(m, zi).wait_recv()
            staged[m, zi] = terms[m, zi * 2 + y] + crossed[m, zi]
            if k:
                term_along(m, zi).start()

    cross_start(0, 1)
    far_cross_start(0)

    def small_along(m, zi):
        ref = smalls.at[m, me]
        return pltpu.make_async_remote_copy(
            src_ref=ref, dst_ref=ref, send_sem=sz_s.at[m, zi], recv_sem=sz_r.at[m, z],
            device_id=(zi * 2 + y, tp), device_id_type=MESH,
        )

    def small_from(m, zi):
        ref = smalls.at[m, zi * 2 + y]
        return pltpu.make_async_remote_copy(
            src_ref=ref, dst_ref=ref, send_sem=sz_s.at[m, zi], recv_sem=sz_r.at[m, zi],
            device_id=(z * 2 + y, tp), device_id_type=MESH,
        )

    def small_cross(m, zi, column):
        ref = smalls.at[m, zi * 2 + column]
        return pltpu.make_async_remote_copy(
            src_ref=ref, dst_ref=ref, send_sem=sy_s.at[m, zi], recv_sem=sy_r.at[m, zi],
            device_id=(z * 2 + 1 - y, tp), device_id_type=MESH,
        )

    for m in range(2):
        here = staged[m, z]
        for k in range(1, depth):
            term_from(m, (z + k) % depth).wait_recv()
            here = here + landed[m, (z + k) % depth]
        first_m = 0.8 * first[m] + 0.2 * here
        second_m = 0.9 * second[m] + 0.1 * here * here
        first_new[m] = first_m
        second_new[m] = second_m
        smalls[m, me] = first_m / (jnp.sqrt(second_m) + 1e-08)
        for k in range(1, depth):
            small_along(m, (z + k) % depth).start()
        small_cross(m, z, y).start()
    for m in range(2):
        for k in range(1, depth):
            zi = (z + k) % depth
            small_from(m, zi).wait_recv()
            small_cross(m, zi, y).start()

    def send_square(m, k):
        return pltpu.make_async_remote_copy(
            src_ref=squares.at[m, tp], dst_ref=squares.at[m, tp], send_sem=norm_s.at[m, k], recv_sem=norm_r.at[m, k],
            device_id=(me, (tp + k) % tps), device_id_type=MESH,
        )

    def recv_square(m, k):
        ref = squares.at[m, (tp + tps - k) % tps]
        return pltpu.make_async_remote_copy(
            src_ref=ref, dst_ref=ref, send_sem=norm_s.at[m, k], recv_sem=norm_r.at[m, k],
            device_id=(me, tp), device_id_type=MESH,
        )

    cross_start(1, 0)
    cross_start(1, 1)
    far_cross_start(1)

    def chunk_ref(block, c):
        return copies.at[c // 2, block, pl.ds(c % 2 * half, half)]

    late = Late(place, 4, chunk_ref, gather_refs[8:])
    beside = z * 2 + 1 - y
    for m in range(2):
        for k in range(depth):
            small_cross(m, (z + k) % depth, 1 - y).wait_recv()
        high, rest = parts_of(smalls[m].reshape(n * slim, smalls.shape[3]))

        def full_of(block):
            factor = factors[m, block]
            return dot(factor, high) + dot(factor, rest)

        total = None
        for block in range(n):
            full = full_of(block)
            square = jnp.sum((full * full).reshape(rows // 8, 8, full.shape[1]), axis=0)
            total = square if total is None else total + square
        squares[m, tp] = total
        for k in range(1, tps):
            send_square(m, k).start()
        update[m] = full_of(me)
        ahead[m, 0] = full_of(jnp.where(at_end, far * 2 + y, beside))
        if m == 0:
            @pl.when(at_end)
            def _():
                ahead[m, 1] = full_of(far * 2 + 1 - y)

    for m in range(2):
        for k in range(1, tps):
            recv_square(m, k).wait_recv()
        mean = jnp.sum(jnp.sum(squares[m], axis=0), keepdims=True) / entries
        root = jnp.sqrt(mean + 1e-06)
        new_update = update[m] / root
        new_weight = weights[m] - 0.02 * new_update
        copies[m, me] = new_weight.astype(BF16)
        for c in range(2 * m, 2 * m + 2):
            late.start_own(c)
        update[m] = new_update
        fresh[m] = new_weight

        @pl.when(middle)
        def _():
            for c in range(2):
                early_cross(m, c).wait_recv()
            copies[m, beside] = (early[0, m] - 0.02 * (ahead[m, 0] / root)).astype(BF16)
            for c in range(2 * m, 2 * m + 2):
                late.start_beside(c)

        @pl.when(at_end)
        def _():
            for c in range(2):
                if m == 0:
                    far_cross(c).wait_recv()
                else:
                    early_far(m, c).wait_recv()
            copies[m, far * 2 + y] = (early[0, m] - 0.02 * (ahead[m, 0] / root)).astype(BF16)
            if m == 0:
                copies[m, far * 2 + 1 - y] = (early[1, m] - 0.02 * (ahead[m, 1] / root)).astype(BF16)
            for c in range(2 * m, 2 * m + 2):
                late.start_far(c)

    late.relay()

    @pl.when(middle)
    def _():
        for m in range(2):
            for c in range(2):
                early_cross(m, c).wait_send()

    @pl.when(at_end)
    def _():
        for c in range(2):
            far_cross(c).wait_send()
            for m in range(2):
                early_far(m, c).wait_send()

    gather.finish()
    late.finish()
    for k in range(1, n):
        for c in range(2):
            hand(side, (me + k) % n, c).wait_send()
    for m in range(2):
        for k in range(depth):
            zi = (z + k) % depth
            term_cross(m, zi).wait_send()
            small_cross(m, zi, y).wait_send()
            if k:
                term_along(m, zi).wait_send()
                small_along(m, zi).wait_send()
        for k in range(1, tps):
            send_square(m, k).wait_send()


def write_kernel(update, fresh, copies, first_new, second_new, *refs):
    outs, sem = refs[:-1], refs[-1]
    started = []
    for i, source in enumerate((update, fresh, copies, first_new, second_new)):
        for m in range(2):
            copy = pltpu.make_async_copy(source.at[m], outs[2 * i + m], sem.at[2 * i + m])
            copy.start()
            started.append(copy)
    for copy in started:
        copy.wait()


def kernel_form(n, tps, saved_input, cot_inproj, cot_outproj, factor_inproj, *others):
    tokens, wide = saved_input.shape
    columns = cot_inproj.shape[1]
    rows, rank = factor_inproj.shape
    slim = rank // n
    depth = n // 2
    entries = float(wide * columns * tps)
    dma = pltpu.SemaphoreType.DMA
    vmem = pl.BlockSpec(memory_space=pltpu.VMEM)
    anywhere = pl.BlockSpec(memory_space=pl.ANY)
    far = pl.BlockSpec(memory_space=pltpu.HBM)
    shape = jax.ShapeDtypeStruct
    results = pl.pallas_call(
        functools.partial(kernel, n, tps, entries),
        out_shape=(
            shape((2, rows, columns), F32), shape((2, rows, columns), F32),
            shape((2, n, rows, columns), BF16),
            shape((2, slim, columns), F32), shape((2, slim, columns), F32),
        ),
        in_specs=[far] * 11,
        out_specs=[vmem] * 5,
        scratch_shapes=[
            pltpu.VMEM((tokens, wide), BF16),
            pltpu.VMEM((2, tokens, columns), BF16),
            pltpu.VMEM((2, n, rows, rank), BF16),
            pltpu.VMEM((2, rows, columns), F32),
            pltpu.VMEM((2, slim, columns), F32),
            pltpu.VMEM((2, slim, columns), F32),
            pltpu.VMEM((2, tokens, rank), F32),
            pltpu.VMEM((2, n, slim, columns), F32),
            pltpu.VMEM((2, depth, slim, columns), F32),
            pltpu.VMEM((2, depth, slim, columns), F32),
            pltpu.VMEM((2, depth, slim, columns), F32),
            pltpu.VMEM((2, n, slim, columns), F32),
            pltpu.VMEM((2, tps, 8, columns), F32),
            pltpu.VMEM((2, 2, rows, columns), F32),
            pltpu.VMEM((2, 2, rows, columns), F32),
            *[dma((2, 2))] * 4,
            dma((11,)),
            dma((n, 2)), dma((n, 2)),
            *[dma((2, depth))] * 8,
            dma((2, tps)), dma((2, tps)),
            *gather_sems(depth, 2), *gather_sems(depth, 4),
        ],
        compiler_params=pltpu.CompilerParams(collective_id=0, has_side_effects=True, vmem_limit_bytes=40 * 2**20),
    )(*[pltpu.with_memory_space_constraint(x, pltpu.HBM) for x in (saved_input, cot_inproj, cot_outproj, factor_inproj, *others)])
    update, fresh, copies, first_new, second_new = results
    copies = copies.reshape(2, n * rows, columns)
    return pl.pallas_call(
        write_kernel,
        out_shape=(
            *[shape((rows, columns), F32)] * 4, *[shape((n * rows, columns), BF16)] * 2, *[shape((slim, columns), F32)] * 4,
        ),
        in_specs=[anywhere] * 5,
        out_specs=[far] * 10,
        scratch_shapes=[dma((10,))],
        compiler_params=pltpu.CompilerParams(vmem_limit_bytes=2**20),
    )(update, fresh, copies, first_new, second_new)


def on_device(saved_input, cot_inproj, cot_outproj, factor_inproj, *others):
    n, tps = lax.axis_size("fs"), lax.axis_size("tp")
    rows, rank = factor_inproj.shape
    if n % 2 == 0 and n == 8 and tps % 2 == 0 and rank % (8 * n) == 0 and rows % 128 == 0 and cot_inproj.shape[1] % 128 == 0:
        return kernel_form(n, tps, saved_input, cot_inproj, cot_outproj, factor_inproj, *others)
    return plain_form(saved_input, cot_inproj, cot_outproj, factor_inproj, *others)


def solution(mesh):
    return jax.shard_map(
        on_device,
        mesh=mesh,
        in_specs=(
            P("fs", None),
            P("fs", "tp"),
            P("fs", "tp"),
            P("fs", None),
            P("fs", None),
            P("fs", "tp"),
            P("fs", "tp"),
            P("fs", "tp"),
            P("fs", "tp"),
            P("fs", "tp"),
            P("fs", "tp"),
        ),
        out_specs=(
            P("fs", "tp"),
            P("fs", "tp"),
            P("fs", "tp"),
            P("fs", "tp"),
            P(None, "tp"),
            P(None, "tp"),
            P("fs", "tp"),
            P("fs", "tp"),
            P("fs", "tp"),
            P("fs", "tp"),
        ),
        check_vma=False,
    )
```

```python
import functools

import jax
import jax.numpy as jnp
from jax import lax
from jax.experimental import pallas as pl
from jax.experimental.pallas import tpu as pltpu
from jax.sharding import PartitionSpec as P


def contract_rows(left, right, precision):
    return lax.dot_general(
        left,
        right,
        (((0,), (0,)), ((), ())),
        precision=precision,
        preferred_element_type=jnp.float32,
    )


def plain_form(
    saved_input,
    cot_inproj,
    cot_outproj,
    factor_inproj,
    factor_outproj,
    weight_inproj,
    weight_outproj,
    first_inproj,
    first_outproj,
    second_inproj,
    second_outproj,
):
    highest = lax.Precision.HIGHEST
    pieces = (
        lax.all_gather(factor_inproj, "fs", axis=0, tiled=True),
        lax.all_gather(factor_outproj, "fs", axis=0, tiled=True),
    )
    mapped_in = jnp.dot(saved_input, pieces[0], preferred_element_type=jnp.float32)
    mapped_out = jnp.dot(saved_input, pieces[1], preferred_element_type=jnp.float32)
    term_in = contract_rows(mapped_in, cot_inproj.astype(jnp.float32), highest)
    term_out = contract_rows(mapped_out, cot_outproj.astype(jnp.float32), highest)
    projected_in, projected_out = (
        lax.psum_scatter(term_in, "fs", scatter_dimension=0, tiled=True),
        lax.psum_scatter(term_out, "fs", scatter_dimension=0, tiled=True),
    )
    first_in_new = 0.8 * first_inproj + 0.2 * projected_in
    first_out_new = 0.8 * first_outproj + 0.2 * projected_out
    second_in_new = 0.9 * second_inproj + 0.1 * projected_in * projected_in
    second_out_new = 0.9 * second_outproj + 0.1 * projected_out * projected_out
    small_in = first_in_new / (jnp.sqrt(second_in_new) + 1e-08)
    small_out = first_out_new / (jnp.sqrt(second_out_new) + 1e-08)
    wide_in = factor_inproj.astype(jnp.float32)
    wide_out = factor_outproj.astype(jnp.float32)
    pieces = (
        lax.all_gather(small_in, "fs", axis=0, tiled=True),
        lax.all_gather(small_out, "fs", axis=0, tiled=True),
    )
    full_in = jnp.dot(wide_in, pieces[0], precision=highest)
    full_out = jnp.dot(wide_out, pieces[1], precision=highest)
    square_in, square_out = lax.psum(
        (jnp.sum(full_in * full_in), jnp.sum(full_out * full_out)), ("fs", "tp")
    )
    entries = float(full_in.shape[0] * full_in.shape[1] * lax.axis_size("fs") * lax.axis_size("tp"))
    update_in = full_in / jnp.sqrt(square_in / entries + 1e-06)
    update_out = full_out / jnp.sqrt(square_out / entries + 1e-06)
    fresh_in = weight_inproj - 0.02 * update_in
    fresh_out = weight_outproj - 0.02 * update_out
    copy_in, copy_out = (
        lax.all_gather(fresh_in.astype(jnp.bfloat16), "fs", axis=0, tiled=True),
        lax.all_gather(fresh_out.astype(jnp.bfloat16), "fs", axis=0, tiled=True),
    )
    return (
        update_in,
        update_out,
        fresh_in,
        fresh_out,
        copy_in,
        copy_out,
        first_in_new,
        first_out_new,
        second_in_new,
        second_out_new,
    )


MESH = pl.DeviceIdType.MESH
F32, BF16 = jnp.float32, jnp.bfloat16


def parts_of(x):
    high = x.astype(BF16)
    return high, (x - high.astype(F32)).astype(BF16)


def dot(a, b):
    return jnp.dot(a, b, preferred_element_type=F32)


class Late:
    def __init__(self, place, chunks, ref_of, sems):
        self.z, self.y, self.tp, self.depth = place
        self.chunks, self.ref_of = chunks, ref_of
        self.up_s, self.up_r, self.dn_s, self.dn_r, self.y_s, self.y_r, self.x_s, self.x_r = sems
        self.last = self.depth - 1
        self.at_end = (self.z == 0) | (self.z == self.last)
        self.far = self.last - self.z
        self.inner = jnp.where(self.z == 0, 1, self.last - 1)
        self.outer = jnp.where(self.z == 1, 0, self.last)

    def second(self, c):
        return c >= self.chunks // 2

    def copy(self, zi, yi, c, s_sem, r_sem, to_z, to_y):
        ref = self.ref_of(zi * 2 + yi, c)
        return pltpu.make_async_remote_copy(
            src_ref=ref, dst_ref=ref, send_sem=s_sem, recv_sem=r_sem,
            device_id=(to_z * 2 + to_y, self.tp), device_id_type=MESH,
        )

    def up(self, s, c):
        return self.copy(self.z - s, self.y, c, self.up_s.at[s, c], self.up_r.at[s, c], self.z + 1, self.y)

    def down(self, s, c):
        return self.copy(self.z + s, self.y, c, self.dn_s.at[s, c], self.dn_r.at[s, c], self.z - 1, self.y)

    def from_below(self, s, c):
        return self.copy(self.z - 1 - s, self.y, c, self.up_s.at[s, c], self.up_r.at[s, c], self.z, self.y)

    def from_above(self, s, c):
        return self.copy(self.z + 1 + s, self.y, c, self.dn_s.at[s, c], self.dn_r.at[s, c], self.z, self.y)

    def across(self, zi, c):
        return self.copy(zi, self.y, c, self.y_s.at[zi, c], self.y_r.at[zi, c], self.z, 1 - self.y)

    def from_across(self, zi, c):
        return self.copy(zi, 1 - self.y, c, self.y_s.at[zi, c], self.y_r.at[zi, c], self.z, self.y)

    def beside(self, zi, c, to_z):
        return self.copy(zi, 1 - self.y, c, self.x_s.at[c], self.x_r.at[c], to_z, self.y)

    def crosses(self, zi, c):
        gap = jnp.abs(self.z - zi)
        near = gap < self.last
        if self.second(c):
            near = near & (gap != 1)
        return jnp.where(self.at_end, near, gap == 1)

    def goes_up(self, s):
        return (self.z - s >= 0) & (self.z < self.last)

    def goes_down(self, s):
        return (self.z + s <= self.last) & (self.z >= 1)

    def start_own(self, c):
        @pl.when(self.goes_up(0))
        def _():
            self.up(0, c).start()

        @pl.when(self.goes_down(0))
        def _():
            self.down(0, c).start()

        @pl.when(self.at_end)
        def _():
            self.across(self.z, c).start()

    def start_far(self, c):
        self.beside(self.far, c, self.inner).start()

    def start_beside(self, c):
        if self.second(c):
            self.beside(self.z, c, self.outer).start()

    def hand_on(self, zi, c):
        @pl.when(self.crosses(zi, c))
        def _():
            self.across(zi, c).start()

    def relay(self):
        z, depth = self.z, self.depth
        for s in range(1, depth - 1):
            for c in range(self.chunks):
                @pl.when(z - s >= 0)
                def _():
                    self.from_below(s - 1, c).wait_recv()
                    if s < depth - 2:
                        @pl.when(z + 1 < depth)
                        def _():
                            self.up(s, c).start()
                    self.hand_on(z - s, c)

                @pl.when(z + s < depth)
                def _():
                    self.from_above(s - 1, c).wait_recv()
                    if s < depth - 2:
                        @pl.when(z >= 1)
                        def _():
                            self.down(s, c).start()
                    self.hand_on(z + s, c)
        for c in range(self.chunks):
            for zi in range(depth):
                @pl.when(self.crosses(zi, c))
                def _():
                    self.from_across(zi, c).wait_recv()

            @pl.when(jnp.logical_not(self.at_end))
            def _():
                self.from_beside(self.last - self.outer, c).wait_recv()

            if self.second(c):
                @pl.when(self.at_end)
                def _():
                    self.from_beside(self.inner, c).wait_recv()

    def from_beside(self, zi, c):
        return self.copy(zi, 1 - self.y, c, self.x_s.at[c], self.x_r.at[c], self.z, self.y)

    def finish(self):
        for c in range(self.chunks):
            for s in range(self.depth - 2):
                @pl.when(self.goes_up(s))
                def _():
                    self.up(s, c).wait_send()

                @pl.when(self.goes_down(s))
                def _():
                    self.down(s, c).wait_send()
            for zi in range(self.depth):
                @pl.when(self.crosses(zi, c))
                def _():
                    self.across(zi, c).wait_send()

            @pl.when(self.at_end)
            def _():
                self.beside(self.far, c, self.inner).wait_send()

            if self.second(c):
                @pl.when(jnp.logical_not(self.at_end))
                def _():
                    self.beside(self.z, c, self.outer).wait_send()


def gather_sems(depth, chunks):
    dma = pltpu.SemaphoreType.DMA
    return [dma((depth - 1, chunks))] * 4 + [dma((depth, chunks))] * 2 + [dma((chunks,))] * 2


def kernel(
    n, tps, entries,
    saved_hbm, cot_in_hbm, cot_out_hbm, factor_in_hbm, factor_out_hbm, weight_in_hbm, weight_out_hbm,
    first_in_hbm, first_out_hbm, second_in_hbm, second_out_hbm,
    update, fresh, copies, first_new, second_new,
    saved, cots, cotx, factors, weights, first, second, moment, moment_new, mapped, terms, crossed, staged, landed,
    smalls, swapped, squares, early, ahead,
    load_sem, fz_s, fz_r, fy_s, fy_r, pair_s, pair_r, cot_s, cot_r, mom_s, mom_r, new_s, new_r, fx_s, fx_r, sx_s, sx_r,
    wy_s, wy_r, wz_s, wz_r, ty_s, ty_r, tz_s, tz_r, sz_s, sz_r, sy_s, sy_r, norm_s, norm_r, *gather_refs,
):
    me, tp = lax.axis_index("fs"), lax.axis_index("tp")
    z, y = me // 2, me % 2
    depth = n // 2
    last = depth - 1
    core, mine = tp % 2, tp // 2
    other = 1 - mine
    matrix = (mine, other)
    partner = mine * 2 + 1 - core
    opposite = other * 2 + core
    rows = factors.shape[2]
    half = rows // 2
    slim = first.shape[1]
    beside = z * 2 + 1 - y
    at_end = (z == 0) | (z == last)
    middle = jnp.logical_not(at_end)
    far = last - z

    barrier = pltpu.get_barrier_semaphore()
    for k in range(1, depth):
        pl.semaphore_signal(barrier, inc=1, device_id=((z + k) % depth * 2 + y, tp), device_id_type=MESH)
    pl.semaphore_signal(barrier, inc=1, device_id=(beside, tp), device_id_type=MESH)
    for k in range(1, tps):
        pl.semaphore_signal(barrier, inc=1, device_id=(me, (tp + k) % tps), device_id_type=MESH)

    loads = [
        pltpu.make_async_copy(source, target, load_sem.at[i])
        for i, (source, target) in enumerate((
            (factor_in_hbm, factors.at[0, me]), (factor_out_hbm, factors.at[1, me]),
            (cot_in_hbm, cots.at[0]), (cot_out_hbm, cots.at[1]),
            (saved_hbm, saved),
            (weight_in_hbm, weights.at[0]), (weight_out_hbm, weights.at[1]),
            (first_in_hbm, first.at[0]), (first_out_hbm, first.at[1]),
            (second_in_hbm, second.at[0]), (second_out_hbm, second.at[1]),
        ))
    ]
    for load in loads:
        load.start()
    loads[0].wait()
    loads[1].wait()
    pl.semaphore_wait(barrier, depth + tps - 1)

    def send(source, target, s_sem, r_sem, to_fs, to_tp):
        return pltpu.make_async_remote_copy(
            src_ref=source, dst_ref=target, send_sem=s_sem, recv_sem=r_sem,
            device_id=(to_fs, to_tp), device_id_type=MESH,
        )

    def factor_part(block):
        return factors.at[mine, block, pl.ds(core * half, half)]

    def factor_along(zi):
        ref = factor_part(me)
        return send(ref, ref, fz_s.at[zi], fz_r.at[z], zi * 2 + y, tp)

    def factor_from(zi):
        ref = factor_part(zi * 2 + y)
        return send(ref, ref, fz_s.at[zi], fz_r.at[zi], me, tp)

    def factor_cross(zi, column):
        ref = factor_part(zi * 2 + column)
        return send(ref, ref, fy_s.at[zi], fy_r.at[zi], beside, tp)

    def hand(block):
        ref = factor_part(block)
        return send(ref, ref, pair_s.at[block], pair_r.at[block], me, partner)

    def handed(block):
        ref = factors.at[mine, block, pl.ds((1 - core) * half, half)]
        return send(ref, ref, pair_s.at[block], pair_r.at[block], me, partner)

    near_one = jnp.where(z % 2 == 0, 1, last - 1)
    far_one = jnp.where(z < depth // 2, last, 0)
    third = jnp.where(z == 0, last - 1, jnp.where(z == last, 1, jnp.where(z == 1, 0, last)))
    factor_along(jnp.where(at_end, far_one, near_one)).start()
    factor_cross(z, y).start()
    factor_along(jnp.where(at_end, third, far_one)).start()
    factor_along(jnp.where(at_end, near_one, third)).start()

    loads[2].wait()
    loads[3].wait()
    cot_swap = send(cots.at[other], cotx, cot_s, cot_r, me, opposite)
    cot_swap.start()

    part_of = lambda c: pl.ds(c * half, half)

    def early_cross(o, c):
        return send(weights.at[matrix[o], part_of(c)], early.at[0, o, part_of(c)], wy_s.at[o, c], wy_r.at[o, c], beside, tp)

    def early_far(o, c):
        return send(
            weights.at[matrix[o], part_of(c)], early.at[0, o, part_of(c)], wz_s.at[o, c], wz_r.at[o, c], far * 2 + y, tp
        )

    def far_cross(o, c):
        return send(early.at[0, o, part_of(c)], early.at[1, o, part_of(c)], wy_s.at[o, c], wy_r.at[o, c], beside, tp)

    def early_start(o, c):
        @pl.when(middle)
        def _():
            early_cross(o, c).start()

    def far_start(o, c):
        @pl.when(at_end)
        def _():
            early_far(o, c).wait_recv()
            far_cross(o, c).start()

    loads[5].wait()
    loads[6].wait()

    @pl.when(at_end)
    def _():
        for o in range(2):
            for c in range(2):
                early_far(o, c).start()

    loads[4].wait()

    def map_block(block, first_one=False):
        piece = saved[:, pl.ds(pl.multiple_of(block * rows, rows), rows)]
        product = dot(piece, factors[mine, block])
        mapped[...] = product if first_one else mapped[...] + product

    def map_handed(block):
        handed(block).wait_recv()
        map_block(block)

    def take_along(zi):
        factor_from(zi).wait_recv()
        factor_cross(zi, y).start()
        hand(zi * 2 + y).start()

    def take_cross(zi):
        factor_cross(zi, 1 - y).wait_recv()
        hand(zi * 2 + 1 - y).start()

    map_block(me, True)
    take_along(near_one)
    take_cross(z)
    take_along(far_one)
    map_handed(near_one * 2 + y)
    map_handed(beside)
    take_along(third)
    take_cross(near_one)
    early_start(0, 0)
    early_start(0, 1)
    map_handed(far_one * 2 + y)
    map_handed(near_one * 2 + 1 - y)
    take_cross(far_one)
    map_handed(third * 2 + y)
    map_handed(far_one * 2 + 1 - y)
    take_cross(third)
    for load in loads[7:]:
        load.wait()
    moment_swap = [
        send(source.at[other], moment.at[i], mom_s.at[i], mom_r.at[i], me, opposite) for i, source in enumerate((first, second))
    ]
    for copy in moment_swap:
        copy.start()
    needed = (jnp.where(at_end, far * 2 + y, beside), jnp.where(at_end, far * 2 + 1 - y, beside))

    def factor_swap(i, m):
        ref = factors.at[m, needed[i]]
        return send(ref, ref, fx_s.at[i], fx_r.at[i], me, opposite)

    map_handed(third * 2 + 1 - y)

    def term_cross(s, zi):
        return send(terms.at[s, zi * 2 + 1 - y], crossed.at[s, zi], ty_s.at[s, zi], ty_r.at[s, zi], beside, tp)

    def term_along(s, zi):
        return send(staged.at[s, zi], landed.at[s, z], tz_s.at[s, zi], tz_r.at[s, z], zi * 2 + y, tp)

    def term_from(s, zi):
        return send(staged.at[s, z], landed.at[s, zi], tz_s.at[s, z], tz_r.at[s, zi], me, tp)

    order = [k % depth for k in range(1, depth + 1)]
    high, rest = parts_of(mapped[...].T)
    for s in range(2):
        if s == 0:
            cot = cots[mine]
        else:
            cot_swap.wait_recv()
            cot = cotx[...]
        term = dot(high, cot) + dot(rest, cot)
        terms[s] = term.reshape(n, slim, term.shape[1])
        for k in order:
            term_cross(s, (z + k) % depth).start()
    factor_swap(0, mine).start()

    @pl.when(at_end)
    def _():
        factor_swap(1, mine).start()

    for s in range(2):
        for k in order:
            zi = (z + k) % depth
            term_cross(s, zi).wait_recv()
            staged[s, zi] = terms[s, zi * 2 + y] + crossed[s, zi]
            if k:
                term_along(s, zi).start()
    early_start(1, 0)
    far_start(0, 0)
    far_start(0, 1)

    def small_along(s, zi):
        ref = smalls.at[s, me]
        return send(ref, ref, sz_s.at[s, zi], sz_r.at[s, z], zi * 2 + y, tp)

    def small_from(s, zi):
        ref = smalls.at[s, zi * 2 + y]
        return send(ref, ref, sz_s.at[s, zi], sz_r.at[s, zi], me, tp)

    def small_cross(s, zi, column):
        ref = smalls.at[s, zi * 2 + column]
        return send(ref, ref, sy_s.at[s, zi], sy_r.at[s, zi], beside, tp)

    def small_swap(block):
        return send(smalls.at[1, block], swapped.at[block], sx_s.at[block], sx_r.at[block], me, opposite)

    def new_swap(i):
        return send(moment_new.at[i], (first_new, second_new)[i].at[mine], new_s.at[i], new_r.at[i], me, opposite)

    for s in range(2):
        here = staged[s, z]
        for k in range(1, depth):
            term_from(s, (z + k) % depth).wait_recv()
            here = here + landed[s, (z + k) % depth]
        if s == 0:
            old_first, old_second = first[mine], second[mine]
        else:
            for copy in moment_swap:
                copy.wait_recv()
            old_first, old_second = moment[0], moment[1]
        new_first = 0.8 * old_first + 0.2 * here
        new_second = 0.9 * old_second + 0.1 * here * here
        smalls[s, me] = new_first / (jnp.sqrt(new_second) + 1e-08)
        for k in range(1, depth):
            small_along(s, (z + k) % depth).start()
        small_cross(s, z, y).start()
        if s == 0:
            first_new[mine] = new_first
            second_new[mine] = new_second
        else:
            small_swap(me).start()
            moment_new[0] = new_first
            moment_new[1] = new_second
    for s in range(2):
        for k in range(1, depth):
            zi = (z + k) % depth
            small_from(s, zi).wait_recv()
            small_cross(s, zi, y).start()
            if s == 1:
                small_swap(zi * 2 + y).start()
    early_start(1, 1)
    far_start(1, 0)
    far_start(1, 1)

    def send_square(k):
        return send(squares.at[tp], squares.at[tp], norm_s.at[k], norm_r.at[k], me, (tp + k) % tps)

    def recv_square(k):
        ref = squares.at[(tp + tps - k) % tps]
        return send(ref, ref, norm_s.at[k], norm_r.at[k], me, tp)

    def full_of(m, block, pieces):
        factor = factors[m, block]
        return dot(factor, pieces[0]) + dot(factor, pieces[1])

    columns = smalls.shape[3]
    total = None
    for s in range(2):
        for k in range(depth):
            zi = (z + k) % depth
            small_cross(s, zi, 1 - y).wait_recv()
            if s == 1:
                small_swap(zi * 2 + 1 - y).start()
        pieces = parts_of(smalls[s].reshape(n * slim, columns))
        for block in range(n):
            full = full_of(mine, block, pieces)
            square = jnp.sum((full * full).reshape(rows // 8, 8, columns), axis=0)
            total = square if total is None else total + square
        if s == 0:
            own_pieces = pieces
    squares[tp] = total
    for k in range(1, tps):
        send_square(k).start()
    for i in range(2):
        new_swap(i).start()

    def chunk_ref(block, c):
        return copies.at[matrix[c // 2], block, pl.ds(c % 2 * half, half)]

    late = Late((z, y, tp, depth), 4, chunk_ref, gather_refs)

    def fill_full(m, pieces):
        update[m] = full_of(m, me, pieces)
        ahead[0] = full_of(m, needed[0], pieces)

        @pl.when(at_end)
        def _():
            ahead[1] = full_of(m, needed[1], pieces)

    def root_of(m):
        mean = jnp.sum(squares[2 * m] + squares[2 * m + 1], keepdims=True) / entries
        return jnp.sqrt(mean + 1e-06)

    for o in range(2):
        m = matrix[o]
        if o == 0:
            fill_full(m, own_pieces)
            for k in range(1, tps):
                recv_square(k).wait_recv()
        else:
            for block in range(n):
                small_swap(block).wait_recv()
            factor_swap(0, other).wait_recv()

            @pl.when(at_end)
            def _():
                factor_swap(1, other).wait_recv()

            fill_full(m, parts_of(swapped[...].reshape(n * slim, columns)))
        root = root_of(m)
        new_update = update[m] / root
        new_weight = weights[m] - 0.02 * new_update
        copies[m, me] = new_weight.astype(BF16)
        for c in range(2 * o, 2 * o + 2):
            late.start_own(c)
        update[m] = new_update
        fresh[m] = new_weight

        @pl.when(middle)
        def _():
            for c in range(2):
                early_cross(o, c).wait_recv()
            copies[m, beside] = (early[0, o] - 0.02 * (ahead[0] / root)).astype(BF16)
            for c in range(2 * o, 2 * o + 2):
                late.start_beside(c)

        @pl.when(at_end)
        def _():
            for c in range(2):
                far_cross(o, c).wait_recv()
            copies[m, far * 2 + 1 - y] = (early[1, o] - 0.02 * (ahead[1] / root)).astype(BF16)
            for c in range(2 * o, 2 * o + 2):
                late.start_far(c)
            copies[m, far * 2 + y] = (early[0, o] - 0.02 * (ahead[0] / root)).astype(BF16)

    late.relay()
    for i in range(2):
        new_swap(i).wait_recv()

    @pl.when(middle)
    def _():
        for o in range(2):
            for c in range(2):
                early_cross(o, c).wait_send()

    @pl.when(at_end)
    def _():
        for o in range(2):
            for c in range(2):
                far_cross(o, c).wait_send()
                early_far(o, c).wait_send()
        factor_swap(1, mine).wait_send()

    factor_swap(0, mine).wait_send()
    late.finish()
    cot_swap.wait_send()
    for i in range(2):
        moment_swap[i].wait_send()
        new_swap(i).wait_send()
    for k in range(1, n):
        hand((me + k) % n).wait_send()
    for k in range(n):
        small_swap(k).wait_send()
    for k in range(depth):
        zi = (z + k) % depth
        factor_cross(zi, y).wait_send()
        if k:
            factor_along(zi).wait_send()
        for s in range(2):
            term_cross(s, zi).wait_send()
            small_cross(s, zi, y).wait_send()
            if k:
                term_along(s, zi).wait_send()
                small_along(s, zi).wait_send()
    for k in range(1, tps):
        send_square(k).wait_send()


def write_kernel(update, fresh, copies, first_new, second_new, *refs):
    outs, sem = refs[:-1], refs[-1]
    started = []
    for i, source in enumerate((update, fresh, copies, first_new, second_new)):
        for m in range(2):
            copy = pltpu.make_async_copy(source.at[m], outs[2 * i + m], sem.at[2 * i + m])
            copy.start()
            started.append(copy)
    for copy in started:
        copy.wait()


def kernel_form(n, tps, saved_input, cot_inproj, cot_outproj, factor_inproj, *others):
    tokens, wide = saved_input.shape
    columns = cot_inproj.shape[1]
    rows, rank = factor_inproj.shape
    slim = rank // n
    depth = n // 2
    entries = float(wide * columns * tps)
    dma = pltpu.SemaphoreType.DMA
    vmem = pl.BlockSpec(memory_space=pltpu.VMEM)
    anywhere = pl.BlockSpec(memory_space=pl.ANY)
    far = pl.BlockSpec(memory_space=pltpu.HBM)
    shape = jax.ShapeDtypeStruct
    results = pl.pallas_call(
        functools.partial(kernel, n, tps, entries),
        out_shape=(
            shape((2, rows, columns), F32), shape((2, rows, columns), F32),
            shape((2, n, rows, columns), BF16),
            shape((2, slim, columns), F32), shape((2, slim, columns), F32),
        ),
        in_specs=[far] * 11,
        out_specs=[vmem] * 5,
        scratch_shapes=[
            pltpu.VMEM((tokens, wide), BF16),
            pltpu.VMEM((2, tokens, columns), BF16),
            pltpu.VMEM((tokens, columns), BF16),
            pltpu.VMEM((2, n, rows, rank), BF16),
            pltpu.VMEM((2, rows, columns), F32),
            *[pltpu.VMEM((2, slim, columns), F32)] * 4,
            pltpu.VMEM((tokens, rank), F32),
            pltpu.VMEM((2, n, slim, columns), F32),
            *[pltpu.VMEM((2, depth, slim, columns), F32)] * 3,
            pltpu.VMEM((2, n, slim, columns), F32),
            pltpu.VMEM((n, slim, columns), F32),
            pltpu.VMEM((tps, 8, columns), F32),
            pltpu.VMEM((2, 2, rows, columns), F32),
            pltpu.VMEM((2, rows, columns), F32),
            dma((11,)),
            *[dma((depth,))] * 4,
            dma((n,)), dma((n,)),
            dma, dma,
            *[dma((2,))] * 6,
            dma((n,)), dma((n,)),
            *[dma((2, 2))] * 4,
            *[dma((2, depth))] * 8,
            dma((tps,)), dma((tps,)),
            *gather_sems(depth, 4),
        ],
        compiler_params=pltpu.CompilerParams(collective_id=0, has_side_effects=True, vmem_limit_bytes=40 * 2**20),
    )(*[pltpu.with_memory_space_constraint(x, pltpu.HBM) for x in (saved_input, cot_inproj, cot_outproj, factor_inproj, *others)])
    update, fresh, copies, first_new, second_new = results
    copies = copies.reshape(2, n * rows, columns)
    return pl.pallas_call(
        write_kernel,
        out_shape=(
            *[shape((rows, columns), F32)] * 4, *[shape((n * rows, columns), BF16)] * 2, *[shape((slim, columns), F32)] * 4,
        ),
        in_specs=[anywhere] * 5,
        out_specs=[far] * 10,
        scratch_shapes=[dma((10,))],
        compiler_params=pltpu.CompilerParams(vmem_limit_bytes=2**20),
    )(update, fresh, copies, first_new, second_new)


def on_device(saved_input, cot_inproj, cot_outproj, factor_inproj, *others):
    n, tps = lax.axis_size("fs"), lax.axis_size("tp")
    rows, rank = factor_inproj.shape
    if n == 8 and tps == 4 and rank % (8 * n) == 0 and rows % 128 == 0 and cot_inproj.shape[1] % 128 == 0:
        return kernel_form(n, tps, saved_input, cot_inproj, cot_outproj, factor_inproj, *others)
    return plain_form(saved_input, cot_inproj, cot_outproj, factor_inproj, *others)


def solution(mesh):
    return jax.shard_map(
        on_device,
        mesh=mesh,
        in_specs=(
            P("fs", None),
            P("fs", "tp"),
            P("fs", "tp"),
            P("fs", None),
            P("fs", None),
            P("fs", "tp"),
            P("fs", "tp"),
            P("fs", "tp"),
            P("fs", "tp"),
            P("fs", "tp"),
            P("fs", "tp"),
        ),
        out_specs=(
            P("fs", "tp"),
            P("fs", "tp"),
            P("fs", "tp"),
            P("fs", "tp"),
            P(None, "tp"),
            P(None, "tp"),
            P("fs", "tp"),
            P("fs", "tp"),
            P("fs", "tp"),
            P("fs", "tp"),
        ),
        check_vma=False,
    )
```

```python
import functools

import jax
import jax.numpy as jnp
from jax import lax
from jax.experimental import pallas as pl
from jax.experimental.pallas import tpu as pltpu
from jax.sharding import PartitionSpec as P


def contract_rows(left, right, precision):
    return lax.dot_general(
        left,
        right,
        (((0,), (0,)), ((), ())),
        precision=precision,
        preferred_element_type=jnp.float32,
    )


def plain_form(
    saved_input,
    cot_inproj,
    cot_outproj,
    factor_inproj,
    factor_outproj,
    weight_inproj,
    weight_outproj,
    first_inproj,
    first_outproj,
    second_inproj,
    second_outproj,
):
    highest = lax.Precision.HIGHEST
    pieces = (
        lax.all_gather(factor_inproj, "fs", axis=0, tiled=True),
        lax.all_gather(factor_outproj, "fs", axis=0, tiled=True),
    )
    mapped_in = jnp.dot(saved_input, pieces[0], preferred_element_type=jnp.float32)
    mapped_out = jnp.dot(saved_input, pieces[1], preferred_element_type=jnp.float32)
    term_in = contract_rows(mapped_in, cot_inproj.astype(jnp.float32), highest)
    term_out = contract_rows(mapped_out, cot_outproj.astype(jnp.float32), highest)
    projected_in, projected_out = (
        lax.psum_scatter(term_in, "fs", scatter_dimension=0, tiled=True),
        lax.psum_scatter(term_out, "fs", scatter_dimension=0, tiled=True),
    )
    first_in_new = 0.8 * first_inproj + 0.2 * projected_in
    first_out_new = 0.8 * first_outproj + 0.2 * projected_out
    second_in_new = 0.9 * second_inproj + 0.1 * projected_in * projected_in
    second_out_new = 0.9 * second_outproj + 0.1 * projected_out * projected_out
    small_in = first_in_new / (jnp.sqrt(second_in_new) + 1e-08)
    small_out = first_out_new / (jnp.sqrt(second_out_new) + 1e-08)
    wide_in = factor_inproj.astype(jnp.float32)
    wide_out = factor_outproj.astype(jnp.float32)
    pieces = (
        lax.all_gather(small_in, "fs", axis=0, tiled=True),
        lax.all_gather(small_out, "fs", axis=0, tiled=True),
    )
    full_in = jnp.dot(wide_in, pieces[0], precision=highest)
    full_out = jnp.dot(wide_out, pieces[1], precision=highest)
    square_in, square_out = lax.psum(
        (jnp.sum(full_in * full_in), jnp.sum(full_out * full_out)), ("fs", "tp")
    )
    entries = float(full_in.shape[0] * full_in.shape[1] * lax.axis_size("fs") * lax.axis_size("tp"))
    update_in = full_in / jnp.sqrt(square_in / entries + 1e-06)
    update_out = full_out / jnp.sqrt(square_out / entries + 1e-06)
    fresh_in = weight_inproj - 0.02 * update_in
    fresh_out = weight_outproj - 0.02 * update_out
    copy_in, copy_out = (
        lax.all_gather(fresh_in.astype(jnp.bfloat16), "fs", axis=0, tiled=True),
        lax.all_gather(fresh_out.astype(jnp.bfloat16), "fs", axis=0, tiled=True),
    )
    return (
        update_in,
        update_out,
        fresh_in,
        fresh_out,
        copy_in,
        copy_out,
        first_in_new,
        first_out_new,
        second_in_new,
        second_out_new,
    )


MESH = pl.DeviceIdType.MESH
F32, BF16 = jnp.float32, jnp.bfloat16


def parts_of(x):
    high = x.astype(BF16)
    return high, (x - high.astype(F32)).astype(BF16)


def dot(a, b):
    return jnp.dot(a, b, preferred_element_type=F32)


class Late:
    def __init__(self, place, chunks, ref_of, sems):
        self.z, self.y, self.tp, self.depth = place
        self.chunks, self.ref_of = chunks, ref_of
        self.up_s, self.up_r, self.dn_s, self.dn_r, self.y_s, self.y_r, self.x_s, self.x_r = sems
        self.last = self.depth - 1
        self.at_end = (self.z == 0) | (self.z == self.last)
        self.far = self.last - self.z
        self.inner = jnp.where(self.z == 0, 1, self.last - 1)
        self.outer = jnp.where(self.z == 1, 0, self.last)

    def copy(self, zi, yi, c, s_sem, r_sem, to_z, to_y):
        ref = self.ref_of(zi * 2 + yi, c)
        return pltpu.make_async_remote_copy(
            src_ref=ref, dst_ref=ref, send_sem=s_sem, recv_sem=r_sem,
            device_id=(to_z * 2 + to_y, self.tp), device_id_type=MESH,
        )

    def up(self, s, c):
        return self.copy(self.z - s, self.y, c, self.up_s.at[s, c], self.up_r.at[s, c], self.z + 1, self.y)

    def down(self, s, c):
        return self.copy(self.z + s, self.y, c, self.dn_s.at[s, c], self.dn_r.at[s, c], self.z - 1, self.y)

    def from_below(self, s, c):
        return self.copy(self.z - 1 - s, self.y, c, self.up_s.at[s, c], self.up_r.at[s, c], self.z, self.y)

    def from_above(self, s, c):
        return self.copy(self.z + 1 + s, self.y, c, self.dn_s.at[s, c], self.dn_r.at[s, c], self.z, self.y)

    def across(self, zi, c):
        return self.copy(zi, self.y, c, self.y_s.at[zi, c], self.y_r.at[zi, c], self.z, 1 - self.y)

    def from_across(self, zi, c):
        return self.copy(zi, 1 - self.y, c, self.y_s.at[zi, c], self.y_r.at[zi, c], self.z, self.y)

    def beside(self, zi, c, to_z):
        return self.copy(zi, 1 - self.y, c, self.x_s.at[c], self.x_r.at[c], to_z, self.y)

    def sidesteps(self, c):
        return 1 <= c and not self.plain(c)

    def plain(self, c):
        return c == self.chunks - 1

    def crosses(self, zi, c):
        gap = jnp.abs(self.z - zi)
        near = gap < self.last
        if self.sidesteps(c):
            near = near & (gap != 1)
        if self.plain(c):
            return (gap >= 0)
        return jnp.where(self.at_end, near, gap == 1)

    def goes_up(self, s):
        return (self.z - s >= 0) & (self.z < self.last)

    def goes_down(self, s):
        return (self.z + s <= self.last) & (self.z >= 1)

    def start_own(self, c):
        @pl.when(self.goes_up(0))
        def _():
            self.up(0, c).start()

        @pl.when(self.goes_down(0))
        def _():
            self.down(0, c).start()

        @pl.when(self.crosses(self.z, c))
        def _():
            self.across(self.z, c).start()

    def start_far(self, c):
        if self.plain(c):
            self.across(self.far, c).start()
        else:
            self.beside(self.far, c, self.inner).start()

    def start_beside(self, c):
        if self.sidesteps(c):
            self.beside(self.z, c, self.outer).start()

    def hand_on(self, zi, c):
        @pl.when(self.crosses(zi, c))
        def _():
            self.across(zi, c).start()

    def relay(self):
        z, depth = self.z, self.depth
        for s in range(1, depth - 1):
            for c in range(self.chunks):
                @pl.when(z - s >= 0)
                def _():
                    self.from_below(s - 1, c).wait_recv()
                    if s < depth - 2:
                        @pl.when(z + 1 < depth)
                        def _():
                            self.up(s, c).start()
                    self.hand_on(z - s, c)

                @pl.when(z + s < depth)
                def _():
                    self.from_above(s - 1, c).wait_recv()
                    if s < depth - 2:
                        @pl.when(z >= 1)
                        def _():
                            self.down(s, c).start()
                    self.hand_on(z + s, c)
        for c in range(self.chunks):
            for zi in range(depth):
                @pl.when(self.crosses(zi, c))
                def _():
                    self.from_across(zi, c).wait_recv()
            if not self.plain(c):
                @pl.when(jnp.logical_not(self.at_end))
                def _():
                    self.from_beside(self.last - self.outer, c).wait_recv()
            if self.sidesteps(c):
                @pl.when(self.at_end)
                def _():
                    self.from_beside(self.inner, c).wait_recv()

    def from_beside(self, zi, c):
        return self.copy(zi, 1 - self.y, c, self.x_s.at[c], self.x_r.at[c], self.z, self.y)

    def finish(self):
        for c in range(self.chunks):
            for s in range(self.depth - 2):
                @pl.when(self.goes_up(s))
                def _():
                    self.up(s, c).wait_send()

                @pl.when(self.goes_down(s))
                def _():
                    self.down(s, c).wait_send()
            for zi in range(self.depth):
                @pl.when(self.crosses(zi, c))
                def _():
                    self.across(zi, c).wait_send()
            if not self.plain(c):
                @pl.when(self.at_end)
                def _():
                    self.beside(self.far, c, self.inner).wait_send()
            if self.sidesteps(c):
                @pl.when(jnp.logical_not(self.at_end))
                def _():
                    self.beside(self.z, c, self.outer).wait_send()


def gather_sems(depth, chunks):
    dma = pltpu.SemaphoreType.DMA
    return [dma((depth - 1, chunks))] * 4 + [dma((depth, chunks))] * 2 + [dma((chunks,))] * 2


def kernel(
    n, tps, entries,
    saved_hbm, cot_in_hbm, cot_out_hbm, factor_in_hbm, factor_out_hbm, weight_in_hbm, weight_out_hbm,
    first_in_hbm, first_out_hbm, second_in_hbm, second_out_hbm,
    update, fresh, copies, first_new, second_new,
    saved, cots, cotx, factors, weights, first, second, moment, moment_new, mapped, terms, crossed, staged, landed,
    smalls, swapped, squares, early, ahead,
    load_sem, fz_s, fz_r, fy_s, fy_r, pair_s, pair_r, cot_s, cot_r, mom_s, mom_r, new_s, new_r, fx_s, fx_r, sx_s, sx_r,
    wy_s, wy_r, wz_s, wz_r, ty_s, ty_r, tz_s, tz_r, sz_s, sz_r, sy_s, sy_r, norm_s, norm_r, *gather_refs,
):
    me, tp = lax.axis_index("fs"), lax.axis_index("tp")
    z, y = me // 2, me % 2
    depth = n // 2
    last = depth - 1
    core, mine = tp % 2, tp // 2
    other = 1 - mine
    matrix = (mine, other)
    partner = mine * 2 + 1 - core
    opposite = other * 2 + core
    rows = factors.shape[2]
    half = rows // 2
    slim = first.shape[1]
    beside = z * 2 + 1 - y
    at_end = (z == 0) | (z == last)
    middle = jnp.logical_not(at_end)
    far = last - z

    barrier = pltpu.get_barrier_semaphore()
    for k in range(1, depth):
        pl.semaphore_signal(barrier, inc=1, device_id=((z + k) % depth * 2 + y, tp), device_id_type=MESH)
    pl.semaphore_signal(barrier, inc=1, device_id=(beside, tp), device_id_type=MESH)
    for k in range(1, tps):
        pl.semaphore_signal(barrier, inc=1, device_id=(me, (tp + k) % tps), device_id_type=MESH)

    loads = [
        pltpu.make_async_copy(source, target, load_sem.at[i])
        for i, (source, target) in enumerate((
            (factor_in_hbm, factors.at[0, me]), (factor_out_hbm, factors.at[1, me]),
            (cot_in_hbm, cots.at[0]), (cot_out_hbm, cots.at[1]),
            (saved_hbm, saved),
            (weight_in_hbm, weights.at[0]), (weight_out_hbm, weights.at[1]),
            (first_in_hbm, first.at[0]), (first_out_hbm, first.at[1]),
            (second_in_hbm, second.at[0]), (second_out_hbm, second.at[1]),
        ))
    ]
    for load in loads:
        load.start()
    loads[0].wait()
    loads[1].wait()
    pl.semaphore_wait(barrier, depth + tps - 1)

    def send(source, target, s_sem, r_sem, to_fs, to_tp):
        return pltpu.make_async_remote_copy(
            src_ref=source, dst_ref=target, send_sem=s_sem, recv_sem=r_sem,
            device_id=(to_fs, to_tp), device_id_type=MESH,
        )

    def factor_part(block):
        return factors.at[mine, block, pl.ds(core * half, half)]

    def factor_along(zi):
        ref = factor_part(me)
        return send(ref, ref, fz_s.at[zi], fz_r.at[z], zi * 2 + y, tp)

    def factor_from(zi):
        ref = factor_part(zi * 2 + y)
        return send(ref, ref, fz_s.at[zi], fz_r.at[zi], me, tp)

    def factor_cross(zi, column):
        ref = factor_part(zi * 2 + column)
        return send(ref, ref, fy_s.at[zi], fy_r.at[zi], beside, tp)

    def hand(block):
        ref = factor_part(block)
        return send(ref, ref, pair_s.at[block], pair_r.at[block], me, partner)

    def handed(block):
        ref = factors.at[mine, block, pl.ds((1 - core) * half, half)]
        return send(ref, ref, pair_s.at[block], pair_r.at[block], me, partner)

    near_one = jnp.where(z % 2 == 0, 1, last - 1)
    far_one = jnp.where(z < depth // 2, last, 0)
    third = jnp.where(z == 0, last - 1, jnp.where(z == last, 1, jnp.where(z == 1, 0, last)))
    factor_along(near_one).start()
    factor_cross(z, y).start()
    factor_along(third).start()
    factor_along(far_one).start()

    loads[2].wait()
    loads[3].wait()
    cot_swap = send(cots.at[other], cotx, cot_s, cot_r, me, opposite)
    cot_swap.start()

    part_of = lambda c: pl.ds(c * half, half)

    def early_cross(o, c):
        return send(weights.at[matrix[o], part_of(c)], early.at[0, o, part_of(c)], wy_s.at[o, c], wy_r.at[o, c], beside, tp)

    def early_far(o, c):
        return send(
            weights.at[matrix[o], part_of(c)], early.at[0, o, part_of(c)], wz_s.at[o, c], wz_r.at[o, c], far * 2 + y, tp
        )

    def far_cross(o, c):
        return send(early.at[0, o, part_of(c)], early.at[1, o, part_of(c)], wy_s.at[o, c], wy_r.at[o, c], beside, tp)

    def early_start(o, c):
        @pl.when(middle)
        def _():
            early_cross(o, c).start()

    def far_start(o, c):
        @pl.when(at_end)
        def _():
            early_far(o, c).wait_recv()
            far_cross(o, c).start()

    loads[4].wait()

    def map_block(block, first_one=False):
        piece = saved[:, pl.ds(pl.multiple_of(block * rows, rows), rows)]
        product = dot(piece, factors[mine, block])
        mapped[...] = product if first_one else mapped[...] + product

    def map_handed(block):
        handed(block).wait_recv()
        map_block(block)

    def take_along(zi):
        factor_from(zi).wait_recv()
        factor_cross(zi, y).start()
        hand(zi * 2 + y).start()

    def take_cross(zi):
        factor_cross(zi, 1 - y).wait_recv()
        hand(zi * 2 + 1 - y).start()

    map_block(me, True)
    take_along(near_one)
    take_along(third)
    take_cross(z)
    map_handed(near_one * 2 + y)
    take_along(far_one)
    loads[5].wait()
    loads[6].wait()

    @pl.when(at_end)
    def _():
        for o in range(2):
            for c in range(2):
                early_far(o, c).start()

    map_handed(third * 2 + y)
    map_handed(beside)
    take_cross(near_one)
    take_cross(third)
    map_handed(near_one * 2 + 1 - y)
    map_handed(far_one * 2 + y)
    take_cross(far_one)
    map_handed(third * 2 + 1 - y)
    for load in loads[7:]:
        load.wait()
    moment_swap = [
        send(source.at[other], moment.at[i], mom_s.at[i], mom_r.at[i], me, opposite) for i, source in enumerate((first, second))
    ]
    for copy in moment_swap:
        copy.start()
    needed = (jnp.where(at_end, far * 2 + y, beside), jnp.where(at_end, far * 2 + 1 - y, beside))

    def factor_swap(i, m):
        ref = factors.at[m, needed[i]]
        return send(ref, ref, fx_s.at[i], fx_r.at[i], me, opposite)

    map_handed(far_one * 2 + 1 - y)

    def term_cross(s, zi):
        return send(terms.at[s, zi * 2 + 1 - y], crossed.at[s, zi], ty_s.at[s, zi], ty_r.at[s, zi], beside, tp)

    def term_along(s, zi):
        return send(staged.at[s, zi], landed.at[s, z], tz_s.at[s, zi], tz_r.at[s, z], zi * 2 + y, tp)

    def term_from(s, zi):
        return send(staged.at[s, z], landed.at[s, zi], tz_s.at[s, z], tz_r.at[s, zi], me, tp)

    order = [k % depth for k in range(1, depth + 1)]
    high, rest = parts_of(mapped[...].T)
    for s in range(2):
        if s == 0:
            cot = cots[mine]
        else:
            cot_swap.wait_recv()
            cot = cotx[...]
        term = dot(high, cot) + dot(rest, cot)
        terms[s] = term.reshape(n, slim, term.shape[1])
        for k in order:
            term_cross(s, (z + k) % depth).start()
    factor_swap(0, mine).start()

    @pl.when(at_end)
    def _():
        factor_swap(1, mine).start()

    for s in range(2):
        for k in order:
            zi = (z + k) % depth
            term_cross(s, zi).wait_recv()
            staged[s, zi] = terms[s, zi * 2 + y] + crossed[s, zi]
            if k:
                term_along(s, zi).start()
    early_start(0, 0)
    far_start(0, 0)

    def small_along(s, zi):
        ref = smalls.at[s, me]
        return send(ref, ref, sz_s.at[s, zi], sz_r.at[s, z], zi * 2 + y, tp)

    def small_from(s, zi):
        ref = smalls.at[s, zi * 2 + y]
        return send(ref, ref, sz_s.at[s, zi], sz_r.at[s, zi], me, tp)

    def small_cross(s, zi, column):
        ref = smalls.at[s, zi * 2 + column]
        return send(ref, ref, sy_s.at[s, zi], sy_r.at[s, zi], beside, tp)

    def small_swap(block):
        return send(smalls.at[1, block], swapped.at[block], sx_s.at[block], sx_r.at[block], me, opposite)

    def new_swap(i):
        return send(moment_new.at[i], (first_new, second_new)[i].at[mine], new_s.at[i], new_r.at[i], me, opposite)

    for s in range(2):
        here = staged[s, z]
        for k in range(1, depth):
            term_from(s, (z + k) % depth).wait_recv()
            here = here + landed[s, (z + k) % depth]
        if s == 0:
            old_first, old_second = first[mine], second[mine]
        else:
            for copy in moment_swap:
                copy.wait_recv()
            old_first, old_second = moment[0], moment[1]
        new_first = 0.8 * old_first + 0.2 * here
        new_second = 0.9 * old_second + 0.1 * here * here
        smalls[s, me] = new_first / (jnp.sqrt(new_second) + 1e-08)
        for k in range(1, depth):
            small_along(s, (z + k) % depth).start()
        small_cross(s, z, y).start()
        if s == 0:
            first_new[mine] = new_first
            second_new[mine] = new_second
        else:
            small_swap(me).start()
            moment_new[0] = new_first
            moment_new[1] = new_second
    for s in range(2):
        for k in range(1, depth):
            zi = (z + k) % depth
            small_from(s, zi).wait_recv()
            small_cross(s, zi, y).start()
            if s == 1:
                small_swap(zi * 2 + y).start()
    for o, c in ((0, 1), (1, 0)):
        early_start(o, c)
        far_start(o, c)

    def send_square(k):
        return send(squares.at[tp], squares.at[tp], norm_s.at[k], norm_r.at[k], me, (tp + k) % tps)

    def recv_square(k):
        ref = squares.at[(tp + tps - k) % tps]
        return send(ref, ref, norm_s.at[k], norm_r.at[k], me, tp)

    def full_of(m, block, pieces):
        factor = factors[m, block]
        return dot(factor, pieces[0]) + dot(factor, pieces[1])

    columns = smalls.shape[3]
    total = None
    for s in range(2):
        for k in range(depth):
            zi = (z + k) % depth
            small_cross(s, zi, 1 - y).wait_recv()
            if s == 1:
                small_swap(zi * 2 + 1 - y).start()
        pieces = parts_of(smalls[s].reshape(n * slim, columns))
        for block in range(n):
            full = full_of(mine, block, pieces)
            square = jnp.sum((full * full).reshape(rows // 8, 8, columns), axis=0)
            total = square if total is None else total + square
        if s == 0:
            own_pieces = pieces
    squares[tp] = total
    for k in range(1, tps):
        send_square(k).start()
    for i in range(2):
        new_swap(i).start()

    def chunk_ref(block, c):
        return copies.at[matrix[c // 2], block, pl.ds(c % 2 * half, half)]

    late = Late((z, y, tp, depth), 4, chunk_ref, gather_refs)

    def fill_full(m, pieces):
        update[m] = full_of(m, me, pieces)
        ahead[0] = full_of(m, needed[0], pieces)

        @pl.when(at_end)
        def _():
            ahead[1] = full_of(m, needed[1], pieces)

    def root_of(m):
        mean = jnp.sum(squares[2 * m] + squares[2 * m + 1], keepdims=True) / entries
        return jnp.sqrt(mean + 1e-06)

    for o in range(2):
        m = matrix[o]
        if o == 0:
            fill_full(m, own_pieces)
            recv_square((tp + tps - partner) % tps).wait_recv()
        else:
            for k in range(2):
                recv_square((tp + tps - other * 2 - k) % tps).wait_recv()
            for block in range(n):
                small_swap(block).wait_recv()
            factor_swap(0, other).wait_recv()

            @pl.when(at_end)
            def _():
                factor_swap(1, other).wait_recv()

            fill_full(m, parts_of(swapped[...].reshape(n * slim, columns)))
        root = root_of(m)
        new_update = update[m] / root
        new_weight = weights[m] - 0.02 * new_update
        copies[m, me] = new_weight.astype(BF16)
        for c in range(2 * o, 2 * o + 2):
            late.start_own(c)
        update[m] = new_update
        fresh[m] = new_weight

        def fill(block, c, slot):
            copies[m, block, part_of(c)] = (early[slot, o, part_of(c)] - 0.02 * (ahead[slot, part_of(c)] / root)).astype(BF16)

        halves = [c for c in range(2) if not late.plain(2 * o + c)]

        @pl.when(middle)
        def _():
            for c in halves:
                early_cross(o, c).wait_recv()
                fill(beside, c, 0)
                late.start_beside(2 * o + c)

        @pl.when(at_end)
        def _():
            for c in range(2):
                if c in halves:
                    far_cross(o, c).wait_recv()
                    fill(far * 2 + 1 - y, c, 1)
                else:
                    early_far(o, c).wait_recv()
                    fill(far * 2 + y, c, 0)
                late.start_far(2 * o + c)
            for c in halves:
                fill(far * 2 + y, c, 0)

    late.relay()
    for i in range(2):
        new_swap(i).wait_recv()

    @pl.when(middle)
    def _():
        for o, c in ((0, 0), (0, 1), (1, 0)):
            early_cross(o, c).wait_send()

    @pl.when(at_end)
    def _():
        for o, c in ((0, 0), (0, 1), (1, 0), (1, 1)):
            if not late.plain(2 * o + c):
                far_cross(o, c).wait_send()
            early_far(o, c).wait_send()
        factor_swap(1, mine).wait_send()

    factor_swap(0, mine).wait_send()
    late.finish()
    cot_swap.wait_send()
    for i in range(2):
        moment_swap[i].wait_send()
        new_swap(i).wait_send()
    for k in range(1, n):
        hand((me + k) % n).wait_send()
    for k in range(n):
        small_swap(k).wait_send()
    for k in range(depth):
        zi = (z + k) % depth
        factor_cross(zi, y).wait_send()
        if k:
            factor_along(zi).wait_send()
        for s in range(2):
            term_cross(s, zi).wait_send()
            small_cross(s, zi, y).wait_send()
            if k:
                term_along(s, zi).wait_send()
                small_along(s, zi).wait_send()
    for k in range(1, tps):
        send_square(k).wait_send()


def write_kernel(update, fresh, copies, first_new, second_new, *refs):
    outs, sem = refs[:-1], refs[-1]
    started = []
    for i, source in enumerate((update, fresh, copies, first_new, second_new)):
        for m in range(2):
            copy = pltpu.make_async_copy(source.at[m], outs[2 * i + m], sem.at[2 * i + m])
            copy.start()
            started.append(copy)
    for copy in started:
        copy.wait()


def kernel_form(n, tps, saved_input, cot_inproj, cot_outproj, factor_inproj, *others):
    tokens, wide = saved_input.shape
    columns = cot_inproj.shape[1]
    rows, rank = factor_inproj.shape
    slim = rank // n
    depth = n // 2
    entries = float(wide * columns * tps)
    dma = pltpu.SemaphoreType.DMA
    vmem = pl.BlockSpec(memory_space=pltpu.VMEM)
    anywhere = pl.BlockSpec(memory_space=pl.ANY)
    far = pl.BlockSpec(memory_space=pltpu.HBM)
    shape = jax.ShapeDtypeStruct
    results = pl.pallas_call(
        functools.partial(kernel, n, tps, entries),
        out_shape=(
            shape((2, rows, columns), F32), shape((2, rows, columns), F32),
            shape((2, n, rows, columns), BF16),
            shape((2, slim, columns), F32), shape((2, slim, columns), F32),
        ),
        in_specs=[far] * 11,
        out_specs=[vmem] * 5,
        scratch_shapes=[
            pltpu.VMEM((tokens, wide), BF16),
            pltpu.VMEM((2, tokens, columns), BF16),
            pltpu.VMEM((tokens, columns), BF16),
            pltpu.VMEM((2, n, rows, rank), BF16),
            pltpu.VMEM((2, rows, columns), F32),
            *[pltpu.VMEM((2, slim, columns), F32)] * 4,
            pltpu.VMEM((tokens, rank), F32),
            pltpu.VMEM((2, n, slim, columns), F32),
            *[pltpu.VMEM((2, depth, slim, columns), F32)] * 3,
            pltpu.VMEM((2, n, slim, columns), F32),
            pltpu.VMEM((n, slim, columns), F32),
            pltpu.VMEM((tps, 8, columns), F32),
            pltpu.VMEM((2, 2, rows, columns), F32),
            pltpu.VMEM((2, rows, columns), F32),
            dma((11,)),
            *[dma((depth,))] * 4,
            dma((n,)), dma((n,)),
            dma, dma,
            *[dma((2,))] * 6,
            dma((n,)), dma((n,)),
            *[dma((2, 2))] * 4,
            *[dma((2, depth))] * 8,
            dma((tps,)), dma((tps,)),
            *gather_sems(depth, 4),
        ],
        compiler_params=pltpu.CompilerParams(collective_id=0, has_side_effects=True, vmem_limit_bytes=40 * 2**20),
    )(*[pltpu.with_memory_space_constraint(x, pltpu.HBM) for x in (saved_input, cot_inproj, cot_outproj, factor_inproj, *others)])
    update, fresh, copies, first_new, second_new = results
    copies = copies.reshape(2, n * rows, columns)
    return pl.pallas_call(
        write_kernel,
        out_shape=(
            *[shape((rows, columns), F32)] * 4, *[shape((n * rows, columns), BF16)] * 2, *[shape((slim, columns), F32)] * 4,
        ),
        in_specs=[anywhere] * 5,
        out_specs=[far] * 10,
        scratch_shapes=[dma((10,))],
        compiler_params=pltpu.CompilerParams(vmem_limit_bytes=2**20),
    )(update, fresh, copies, first_new, second_new)


def on_device(saved_input, cot_inproj, cot_outproj, factor_inproj, *others):
    n, tps = lax.axis_size("fs"), lax.axis_size("tp")
    rows, rank = factor_inproj.shape
    if n == 8 and tps == 4 and rank % (8 * n) == 0 and rows % 128 == 0 and cot_inproj.shape[1] % 128 == 0:
        return kernel_form(n, tps, saved_input, cot_inproj, cot_outproj, factor_inproj, *others)
    return plain_form(saved_input, cot_inproj, cot_outproj, factor_inproj, *others)


def solution(mesh):
    return jax.shard_map(
        on_device,
        mesh=mesh,
        in_specs=(
            P("fs", None),
            P("fs", "tp"),
            P("fs", "tp"),
            P("fs", None),
            P("fs", None),
            P("fs", "tp"),
            P("fs", "tp"),
            P("fs", "tp"),
            P("fs", "tp"),
            P("fs", "tp"),
            P("fs", "tp"),
        ),
        out_specs=(
            P("fs", "tp"),
            P("fs", "tp"),
            P("fs", "tp"),
            P("fs", "tp"),
            P(None, "tp"),
            P(None, "tp"),
            P("fs", "tp"),
            P("fs", "tp"),
            P("fs", "tp"),
            P("fs", "tp"),
        ),
        check_vma=False,
    )
```

```python
import functools

import jax
import jax.numpy as jnp
from jax import lax
from jax.experimental import pallas as pl
from jax.experimental.pallas import tpu as pltpu
from jax.sharding import PartitionSpec as P


def contract_rows(left, right, precision):
    return lax.dot_general(
        left,
        right,
        (((0,), (0,)), ((), ())),
        precision=precision,
        preferred_element_type=jnp.float32,
    )


def plain_form(
    saved_input,
    cot_inproj,
    cot_outproj,
    factor_inproj,
    factor_outproj,
    weight_inproj,
    weight_outproj,
    first_inproj,
    first_outproj,
    second_inproj,
    second_outproj,
):
    highest = lax.Precision.HIGHEST
    pieces = (
        lax.all_gather(factor_inproj, "fs", axis=0, tiled=True),
        lax.all_gather(factor_outproj, "fs", axis=0, tiled=True),
    )
    mapped_in = jnp.dot(saved_input, pieces[0], preferred_element_type=jnp.float32)
    mapped_out = jnp.dot(saved_input, pieces[1], preferred_element_type=jnp.float32)
    term_in = contract_rows(mapped_in, cot_inproj.astype(jnp.float32), highest)
    term_out = contract_rows(mapped_out, cot_outproj.astype(jnp.float32), highest)
    projected_in, projected_out = (
        lax.psum_scatter(term_in, "fs", scatter_dimension=0, tiled=True),
        lax.psum_scatter(term_out, "fs", scatter_dimension=0, tiled=True),
    )
    first_in_new = 0.8 * first_inproj + 0.2 * projected_in
    first_out_new = 0.8 * first_outproj + 0.2 * projected_out
    second_in_new = 0.9 * second_inproj + 0.1 * projected_in * projected_in
    second_out_new = 0.9 * second_outproj + 0.1 * projected_out * projected_out
    small_in = first_in_new / (jnp.sqrt(second_in_new) + 1e-08)
    small_out = first_out_new / (jnp.sqrt(second_out_new) + 1e-08)
    wide_in = factor_inproj.astype(jnp.float32)
    wide_out = factor_outproj.astype(jnp.float32)
    pieces = (
        lax.all_gather(small_in, "fs", axis=0, tiled=True),
        lax.all_gather(small_out, "fs", axis=0, tiled=True),
    )
    full_in = jnp.dot(wide_in, pieces[0], precision=highest)
    full_out = jnp.dot(wide_out, pieces[1], precision=highest)
    square_in, square_out = lax.psum(
        (jnp.sum(full_in * full_in), jnp.sum(full_out * full_out)), ("fs", "tp")
    )
    entries = float(full_in.shape[0] * full_in.shape[1] * lax.axis_size("fs") * lax.axis_size("tp"))
    update_in = full_in / jnp.sqrt(square_in / entries + 1e-06)
    update_out = full_out / jnp.sqrt(square_out / entries + 1e-06)
    fresh_in = weight_inproj - 0.02 * update_in
    fresh_out = weight_outproj - 0.02 * update_out
    copy_in, copy_out = (
        lax.all_gather(fresh_in.astype(jnp.bfloat16), "fs", axis=0, tiled=True),
        lax.all_gather(fresh_out.astype(jnp.bfloat16), "fs", axis=0, tiled=True),
    )
    return (
        update_in,
        update_out,
        fresh_in,
        fresh_out,
        copy_in,
        copy_out,
        first_in_new,
        first_out_new,
        second_in_new,
        second_out_new,
    )


MESH = pl.DeviceIdType.MESH
F32, BF16 = jnp.float32, jnp.bfloat16


def parts_of(x):
    high = x.astype(BF16)
    return high, (x - high.astype(F32)).astype(BF16)


def dot(a, b):
    return jnp.dot(a, b, preferred_element_type=F32)


END_OWN, MID_OWN, END_FAR = (2, 3), (2, 3), (0, 1)


class Late:
    def __init__(self, place, chunks, ref_of, sems):
        self.z, self.y, self.tp, self.depth = place
        self.chunks, self.ref_of = chunks, ref_of
        self.up_s, self.up_r, self.dn_s, self.dn_r, self.y_s, self.y_r, self.x_s, self.x_r = sems
        self.last = self.depth - 1
        self.at_end = (self.z == 0) | (self.z == self.last)
        self.far = self.last - self.z
        self.inner = jnp.where(self.z == 0, 1, self.last - 1)
        self.outer = jnp.where(self.z == 1, 0, self.last)

    def copy(self, zi, yi, c, s_sem, r_sem, to_z, to_y):
        ref = self.ref_of(zi * 2 + yi, c)
        return pltpu.make_async_remote_copy(
            src_ref=ref, dst_ref=ref, send_sem=s_sem, recv_sem=r_sem,
            device_id=(to_z * 2 + to_y, self.tp), device_id_type=MESH,
        )

    def up(self, s, c):
        return self.copy(self.z - s, self.y, c, self.up_s.at[s, c], self.up_r.at[s, c], self.z + 1, self.y)

    def down(self, s, c):
        return self.copy(self.z + s, self.y, c, self.dn_s.at[s, c], self.dn_r.at[s, c], self.z - 1, self.y)

    def from_below(self, s, c):
        return self.copy(self.z - 1 - s, self.y, c, self.up_s.at[s, c], self.up_r.at[s, c], self.z, self.y)

    def from_above(self, s, c):
        return self.copy(self.z + 1 + s, self.y, c, self.dn_s.at[s, c], self.dn_r.at[s, c], self.z, self.y)

    def across(self, zi, c):
        return self.copy(zi, self.y, c, self.y_s.at[zi, c], self.y_r.at[zi, c], self.z, 1 - self.y)

    def from_across(self, zi, c):
        return self.copy(zi, 1 - self.y, c, self.y_s.at[zi, c], self.y_r.at[zi, c], self.z, self.y)

    def beside(self, k, zi, c, to_z):
        return self.copy(zi, 1 - self.y, c, self.x_s.at[k, c], self.x_r.at[k, c], to_z, self.y)

    def sidesteps(self, c):
        middle = jnp.logical_not(self.at_end)
        cases = []
        if c in END_FAR:
            cases.append((self.at_end, 0, self.far, self.inner, self.last - self.outer))
        if c in END_OWN:
            cases.append((self.at_end, 1, self.z, self.inner, self.outer))
        sent, landed = [(p, k, zi, to) for p, k, zi, to, _ in cases], [(middle, k, zi) for _, k, _, _, zi in cases]
        if c in MID_OWN:
            sent += [(middle, 2, self.z, self.outer), (middle, 3, self.z, self.far)]
            landed += [(self.at_end, 2, self.inner), (middle, 3, self.far)]
        return sent, landed

    def crosses(self, zi, c):
        gap = jnp.abs(self.z - zi)
        own_end, own_middle, far_end = c not in END_OWN, c not in MID_OWN, c not in END_FAR
        from_end = jnp.where(gap == 2, far_end, own_end)
        at_middle = jnp.where((zi == 0) | (zi == self.last), from_end, own_middle)
        at_end = jnp.where(gap == 0, own_end, jnp.where(gap == 1, own_middle, jnp.where(gap == 2, True, far_end)))
        return jnp.where(self.at_end, at_end, at_middle)

    def goes_up(self, s):
        return (self.z - s >= 0) & (self.z < self.last)

    def goes_down(self, s):
        return (self.z + s <= self.last) & (self.z >= 1)

    def start_own(self, c):
        @pl.when(self.goes_up(0))
        def _():
            self.up(0, c).start()

        @pl.when(self.goes_down(0))
        def _():
            self.down(0, c).start()

        @pl.when(self.crosses(self.z, c))
        def _():
            self.across(self.z, c).start()

    def start_beside(self, c, kinds):
        for condition, k, zi, to_z in self.sidesteps(c)[0]:
            if k in kinds:
                @pl.when(condition)
                def _():
                    self.beside(k, zi, c, to_z).start()

    def start_far(self, c):
        if c not in END_FAR:
            self.across(self.far, c).start()

    def hand_on(self, zi, c):
        @pl.when(self.crosses(zi, c))
        def _():
            self.across(zi, c).start()

    def relay(self):
        z, depth = self.z, self.depth
        for s in range(1, depth - 1):
            for c in range(self.chunks):
                @pl.when(z - s >= 0)
                def _():
                    self.from_below(s - 1, c).wait_recv()
                    if s < depth - 2:
                        @pl.when(z + 1 < depth)
                        def _():
                            self.up(s, c).start()
                    self.hand_on(z - s, c)

                @pl.when(z + s < depth)
                def _():
                    self.from_above(s - 1, c).wait_recv()
                    if s < depth - 2:
                        @pl.when(z >= 1)
                        def _():
                            self.down(s, c).start()
                    self.hand_on(z + s, c)
            if s == 1:
                for c in range(self.chunks):
                    self.start_beside(c, (2, 3))
        for c in range(self.chunks):
            for zi in range(depth):
                @pl.when(self.crosses(zi, c))
                def _():
                    self.from_across(zi, c).wait_recv()
            for condition, k, zi in self.sidesteps(c)[1]:
                @pl.when(condition)
                def _():
                    self.beside(k, zi, c, self.z).wait_recv()

    def finish(self):
        for c in range(self.chunks):
            for s in range(self.depth - 2):
                @pl.when(self.goes_up(s))
                def _():
                    self.up(s, c).wait_send()

                @pl.when(self.goes_down(s))
                def _():
                    self.down(s, c).wait_send()
            for zi in range(self.depth):
                @pl.when(self.crosses(zi, c))
                def _():
                    self.across(zi, c).wait_send()
            for condition, k, zi, to_z in self.sidesteps(c)[0]:
                @pl.when(condition)
                def _():
                    self.beside(k, zi, c, to_z).wait_send()


def gather_sems(depth, chunks):
    dma = pltpu.SemaphoreType.DMA
    return [dma((depth - 1, chunks))] * 4 + [dma((depth, chunks))] * 2 + [dma((4, chunks))] * 2


def kernel(
    n, tps, entries,
    saved_hbm, cot_in_hbm, cot_out_hbm, factor_in_hbm, factor_out_hbm, weight_in_hbm, weight_out_hbm,
    first_in_hbm, first_out_hbm, second_in_hbm, second_out_hbm,
    update, fresh, copies, first_new, second_new,
    saved, cots, cotx, factors, weights, first, second, moment, moment_new, mapped, terms, crossed, staged, landed,
    smalls, swapped, squares, early, ahead,
    load_sem, fz_s, fz_r, fy_s, fy_r, pair_s, pair_r, cot_s, cot_r, mom_s, mom_r, new_s, new_r, fx_s, fx_r, sx_s, sx_r,
    vy_s, vy_r, wy_s, wy_r, wz_s, wz_r, ty_s, ty_r, tz_s, tz_r, sz_s, sz_r, sy_s, sy_r, norm_s, norm_r, *gather_refs,
):
    me, tp = lax.axis_index("fs"), lax.axis_index("tp")
    z, y = me // 2, me % 2
    depth = n // 2
    last = depth - 1
    core, mine = tp % 2, tp // 2
    other = 1 - mine
    matrix = (mine, other)
    partner = mine * 2 + 1 - core
    opposite = other * 2 + core
    rows = factors.shape[2]
    half = rows // 2
    slim = first.shape[1]
    beside = z * 2 + 1 - y
    at_end = (z == 0) | (z == last)
    middle = jnp.logical_not(at_end)
    far = last - z

    barrier = pltpu.get_barrier_semaphore()
    for k in range(1, depth):
        pl.semaphore_signal(barrier, inc=1, device_id=((z + k) % depth * 2 + y, tp), device_id_type=MESH)
    pl.semaphore_signal(barrier, inc=1, device_id=(beside, tp), device_id_type=MESH)
    for k in range(1, tps):
        pl.semaphore_signal(barrier, inc=1, device_id=(me, (tp + k) % tps), device_id_type=MESH)

    loads = [
        pltpu.make_async_copy(source, target, load_sem.at[i])
        for i, (source, target) in enumerate((
            (factor_in_hbm, factors.at[0, me]), (factor_out_hbm, factors.at[1, me]),
            (cot_in_hbm, cots.at[0]), (cot_out_hbm, cots.at[1]),
            (saved_hbm, saved),
            (weight_in_hbm, weights.at[0]), (weight_out_hbm, weights.at[1]),
            (first_in_hbm, first.at[0]), (first_out_hbm, first.at[1]),
            (second_in_hbm, second.at[0]), (second_out_hbm, second.at[1]),
        ))
    ]
    for load in loads:
        load.start()
    loads[0].wait()
    loads[1].wait()
    pl.semaphore_wait(barrier, depth + tps - 1)

    def send(source, target, s_sem, r_sem, to_fs, to_tp):
        return pltpu.make_async_remote_copy(
            src_ref=source, dst_ref=target, send_sem=s_sem, recv_sem=r_sem,
            device_id=(to_fs, to_tp), device_id_type=MESH,
        )

    def factor_part(block):
        return factors.at[mine, block, pl.ds(core * half, half)]

    def factor_along(zi):
        ref = factor_part(me)
        return send(ref, ref, fz_s.at[zi], fz_r.at[z], zi * 2 + y, tp)

    def factor_from(zi):
        ref = factor_part(zi * 2 + y)
        return send(ref, ref, fz_s.at[zi], fz_r.at[zi], me, tp)

    def factor_cross(zi, column):
        ref = factor_part(zi * 2 + column)
        return send(ref, ref, fy_s.at[zi], fy_r.at[zi], beside, tp)

    def hand(block):
        ref = factor_part(block)
        return send(ref, ref, pair_s.at[block], pair_r.at[block], me, partner)

    def handed(block):
        ref = factors.at[mine, block, pl.ds((1 - core) * half, half)]
        return send(ref, ref, pair_s.at[block], pair_r.at[block], me, partner)

    near_one = jnp.where(z % 2 == 0, 1, last - 1)
    far_one = jnp.where(z < depth // 2, last, 0)
    third = jnp.where(z == 0, last - 1, jnp.where(z == last, 1, jnp.where(z == 1, 0, last)))
    factor_along(near_one).start()
    factor_cross(z, y).start()
    factor_along(third).start()
    factor_along(far_one).start()

    loads[2].wait()
    loads[3].wait()
    cot_swap = send(cots.at[other], cotx, cot_s, cot_r, me, opposite)
    cot_swap.start()

    part_of = lambda c: pl.ds(c * half, half)

    def early_cross(o, c):
        return send(weights.at[matrix[o], part_of(c)], early.at[2, o, part_of(c)], wy_s.at[o, c], wy_r.at[o, c], beside, tp)

    def early_far(o, c):
        return send(
            weights.at[matrix[o], part_of(c)], early.at[0, o, part_of(c)], wz_s.at[o, c], wz_r.at[o, c], far * 2 + y, tp
        )

    def far_cross(c):
        return send(early.at[0, 0, part_of(c)], early.at[1, 0, part_of(c)], vy_s.at[c], vy_r.at[c], beside, tp)

    def bulk_across(i):
        @pl.when(middle)
        def _():
            for c in MID_OWN[i : i + 1]:
                early_cross(c // 2, c % 2).start()

        @pl.when(at_end)
        def _():
            for c in END_FAR[i : i + 1]:
                early_far(0, c).wait_recv()
                far_cross(c).start()

    loads[4].wait()

    def map_block(block, first_one=False):
        piece = saved[:, pl.ds(pl.multiple_of(block * rows, rows), rows)]
        product = dot(piece, factors[mine, block])
        mapped[...] = product if first_one else mapped[...] + product

    def map_handed(block):
        handed(block).wait_recv()
        map_block(block)

    def take_along(zi):
        factor_from(zi).wait_recv()
        factor_cross(zi, y).start()
        hand(zi * 2 + y).start()

    def take_cross(zi):
        factor_cross(zi, 1 - y).wait_recv()
        hand(zi * 2 + 1 - y).start()

    map_block(me, True)
    take_along(near_one)
    take_along(third)
    take_cross(z)
    map_handed(near_one * 2 + y)
    take_along(far_one)
    loads[5].wait()
    loads[6].wait()

    @pl.when(at_end)
    def _():
        for c in END_OWN:
            early_cross(c // 2, c % 2).start()
        for o, c in ((0, 0), (0, 1), (1, 0)):
            early_far(o, c).start()

    map_handed(third * 2 + y)
    map_handed(beside)
    take_cross(near_one)
    take_cross(third)
    map_handed(near_one * 2 + 1 - y)
    map_handed(far_one * 2 + y)
    take_cross(far_one)
    map_handed(third * 2 + 1 - y)
    for load in loads[7:]:
        load.wait()
    moment_swap = [
        send(source.at[other], moment.at[i], mom_s.at[i], mom_r.at[i], me, opposite) for i, source in enumerate((first, second))
    ]
    for copy in moment_swap:
        copy.start()

    def factor_swap(m, i=0):
        ref = factors.at[m, jnp.where(at_end, far * 2 + y, beside) if i == 0 else beside]
        return send(ref, ref, fx_s.at[i], fx_r.at[i], me, opposite)

    map_handed(far_one * 2 + 1 - y)

    def term_cross(t):
        return send(terms.at[t, 1 - y], crossed.at[t], ty_s.at[t], ty_r.at[t], beside, tp)

    def term_along(t, zi):
        return send(staged.at[t, zi], landed.at[t, z], tz_s.at[t, zi], tz_r.at[t, z], zi * 2 + y, tp)

    def term_from(t, zi):
        return send(staged.at[t, z], landed.at[t, zi], tz_s.at[t, z], tz_r.at[t, zi], me, tp)

    others = range(1, depth)
    piece = slim // 2
    chunks = [(s, q) for s in range(2) for q in range(2)]
    high, rest = parts_of(mapped[...].T)
    for s in range(2):
        if s == 0:
            cot = cots[mine]
        else:
            cot_swap.wait_recv()
            cot = cotx[...]
        term = (dot(high, cot) + dot(rest, cot)).reshape(depth, 2, 2, piece, cot.shape[1])
        for q in range(2):
            for column in range(2):
                terms[2 * s + q, column] = term[:, column, q]
            term_cross(2 * s + q).start()
    factor_swap(mine).start()

    @pl.when(at_end)
    def _():
        factor_swap(mine, 1).start()

    for t in range(4):
        term_cross(t).wait_recv()
        staged[t] = terms[t, y] + crossed[t]
        for k in others:
            term_along(t, (z + k) % depth).start()
    bulk_across(0)

    def small_piece(t, block):
        return smalls.at[t // 2, block, pl.ds(t % 2 * piece, piece)]

    def small_along(t, zi):
        ref = small_piece(t, me)
        return send(ref, ref, sz_s.at[t, zi], sz_r.at[t, z], zi * 2 + y, tp)

    def small_from(t, zi):
        ref = small_piece(t, zi * 2 + y)
        return send(ref, ref, sz_s.at[t, zi], sz_r.at[t, zi], me, tp)

    def small_cross(t, zi, column):
        ref = small_piece(t, zi * 2 + column)
        return send(ref, ref, sy_s.at[t, zi], sy_r.at[t, zi], beside, tp)

    def small_swap(t, block):
        return send(
            small_piece(t, block), swapped.at[block, pl.ds(t % 2 * piece, piece)],
            sx_s.at[t % 2, block], sx_r.at[t % 2, block], me, opposite,
        )

    def new_swap(i):
        return send(moment_new.at[i], (first_new, second_new)[i].at[mine], new_s.at[i], new_r.at[i], me, opposite)

    for t, (s, q) in enumerate(chunks):
        part = pl.ds(q * piece, piece)
        here = staged[t, z]
        for k in others:
            term_from(t, (z + k) % depth).wait_recv()
            here = here + landed[t, (z + k) % depth]
        if s == 0:
            old_first, old_second = first[mine, part], second[mine, part]
        else:
            if q == 0:
                for copy in moment_swap:
                    copy.wait_recv()
            old_first, old_second = moment[0, part], moment[1, part]
        new_first = 0.8 * old_first + 0.2 * here
        new_second = 0.9 * old_second + 0.1 * here * here
        smalls[s, me, part] = new_first / (jnp.sqrt(new_second) + 1e-08)
        for k in others:
            small_along(t, (z + k) % depth).start()
        small_cross(t, z, y).start()
        if s == 0:
            first_new[mine, part] = new_first
            second_new[mine, part] = new_second
        else:
            small_swap(t, me).start()
            moment_new[0, part] = new_first
            moment_new[1, part] = new_second
    for t, (s, q) in enumerate(chunks):
        for k in others:
            zi = (z + k) % depth
            small_from(t, zi).wait_recv()
            small_cross(t, zi, y).start()
            if s == 1:
                small_swap(t, zi * 2 + y).start()
    @pl.when(at_end)
    def _():
        early_far(1, 1).start()

    def send_square(k):
        return send(squares.at[tp], squares.at[tp], norm_s.at[k], norm_r.at[k], me, (tp + k) % tps)

    def recv_square(k):
        ref = squares.at[(tp + tps - k) % tps]
        return send(ref, ref, norm_s.at[k], norm_r.at[k], me, tp)

    def full_of(m, block, pieces):
        factor = factors[m, block]
        return dot(factor, pieces[0]) + dot(factor, pieces[1])

    columns = smalls.shape[3]
    total = None
    for s in range(2):
        for t in (2 * s, 2 * s + 1):
            for k in range(depth):
                zi = (z + k) % depth
                small_cross(t, zi, 1 - y).wait_recv()
                if s == 1:
                    small_swap(t, zi * 2 + 1 - y).start()
        if s == 0:
            bulk_across(1)
        pieces = parts_of(smalls[s].reshape(n * slim, columns))
        for block in range(n):
            full = full_of(mine, block, pieces)
            square = jnp.sum((full * full).reshape(rows // 8, 8, columns), axis=0)
            total = square if total is None else total + square
        if s == 0:
            own_pieces = pieces
    squares[tp] = total
    for k in range(1, tps):
        send_square(k).start()
    for i in range(2):
        new_swap(i).start()

    def chunk_ref(block, c):
        return copies.at[matrix[c // 2], block, pl.ds(c % 2 * half, half)]

    late = Late((z, y, tp, depth), 4, chunk_ref, gather_refs)

    def fill_full(m, pieces, o):
        update[m] = full_of(m, me, pieces)

        @pl.when(at_end)
        def _():
            ahead[0] = full_of(m, far * 2 + y, pieces)
            if o == 0:
                ahead[1] = full_of(m, far * 2 + 1 - y, pieces)
            if any(c // 2 == o for c in END_OWN):
                ahead[2] = full_of(m, beside, pieces)

        if any(c // 2 == o for c in MID_OWN):
            @pl.when(middle)
            def _():
                ahead[2] = full_of(m, beside, pieces)

    def root_of(m):
        mean = jnp.sum(squares[2 * m] + squares[2 * m + 1], keepdims=True) / entries
        return jnp.sqrt(mean + 1e-06)

    for o in range(2):
        m = matrix[o]
        if o == 0:
            fill_full(m, own_pieces, o)
            recv_square((tp + tps - partner) % tps).wait_recv()
        else:
            for block in range(n):
                for t in (2, 3):
                    small_swap(t, block).wait_recv()
            factor_swap(other).wait_recv()

            @pl.when(at_end)
            def _():
                factor_swap(other, 1).wait_recv()

            fill_full(m, parts_of(swapped[...].reshape(n * slim, columns)), o)
            for k in range(2):
                recv_square((tp + tps - other * 2 - k) % tps).wait_recv()
        root = root_of(m)
        new_update = update[m] / root
        new_weight = weights[m] - 0.02 * new_update
        copies[m, me] = new_weight.astype(BF16)
        for c in range(2 * o, 2 * o + 2):
            late.start_own(c)
        update[m] = new_update
        fresh[m] = new_weight

        def fill(block, c, slot):
            copies[m, block, part_of(c)] = (early[slot, o, part_of(c)] - 0.02 * (ahead[slot, part_of(c)] / root)).astype(BF16)

        def fill_beside(c):
            early_cross(o, c % 2).wait_recv()
            fill(beside, c % 2, 2)

        @pl.when(middle)
        def _():
            for c in MID_OWN:
                if c // 2 == o:
                    fill_beside(c)

        @pl.when(at_end)
        def _():
            for c in range(2 * o, 2 * o + 2):
                if c in END_FAR:
                    far_cross(c).wait_recv()
                    fill(far * 2 + 1 - y, c, 1)
                    late.start_beside(c, (0,))
                else:
                    if o == 1:
                        early_far(o, c % 2).wait_recv()
                    fill(far * 2 + y, c % 2, 0)
                    late.start_far(c)
            for c in END_OWN:
                if c // 2 == o:
                    fill_beside(c)
                    late.start_beside(c, (1,))
            for c in END_FAR:
                if c // 2 == o:
                    fill(far * 2 + y, c, 0)

    late.relay()
    for i in range(2):
        new_swap(i).wait_recv()

    @pl.when(middle)
    def _():
        for c in MID_OWN:
            early_cross(c // 2, c % 2).wait_send()

    @pl.when(at_end)
    def _():
        for c in END_OWN:
            early_cross(c // 2, c % 2).wait_send()
        for c in END_FAR:
            far_cross(c).wait_send()
        for o in range(2):
            for c in range(2):
                early_far(o, c).wait_send()

    factor_swap(mine).wait_send()

    @pl.when(at_end)
    def _():
        factor_swap(mine, 1).wait_send()

    late.finish()
    cot_swap.wait_send()
    for i in range(2):
        moment_swap[i].wait_send()
        new_swap(i).wait_send()
    for k in range(1, n):
        hand((me + k) % n).wait_send()
    for k in range(n):
        for t in (2, 3):
            small_swap(t, k).wait_send()
    for k in range(depth):
        zi = (z + k) % depth
        factor_cross(zi, y).wait_send()
        if k:
            factor_along(zi).wait_send()
        for t in range(4):
            if not k:
                term_cross(t).wait_send()
            small_cross(t, zi, y).wait_send()
            if k:
                term_along(t, zi).wait_send()
                small_along(t, zi).wait_send()
    for k in range(1, tps):
        send_square(k).wait_send()


def write_kernel(update, fresh, copies, first_new, second_new, *refs):
    outs, sem = refs[:-1], refs[-1]
    started = []
    for i, source in enumerate((update, fresh, copies, first_new, second_new)):
        for m in range(2):
            copy = pltpu.make_async_copy(source.at[m], outs[2 * i + m], sem.at[2 * i + m])
            copy.start()
            started.append(copy)
    for copy in started:
        copy.wait()


def kernel_form(n, tps, saved_input, cot_inproj, cot_outproj, factor_inproj, *others):
    tokens, wide = saved_input.shape
    columns = cot_inproj.shape[1]
    rows, rank = factor_inproj.shape
    slim = rank // n
    depth = n // 2
    entries = float(wide * columns * tps)
    dma = pltpu.SemaphoreType.DMA
    vmem = pl.BlockSpec(memory_space=pltpu.VMEM)
    anywhere = pl.BlockSpec(memory_space=pl.ANY)
    far = pl.BlockSpec(memory_space=pltpu.HBM)
    shape = jax.ShapeDtypeStruct
    results = pl.pallas_call(
        functools.partial(kernel, n, tps, entries),
        out_shape=(
            shape((2, rows, columns), F32), shape((2, rows, columns), F32),
            shape((2, n, rows, columns), BF16),
            shape((2, slim, columns), F32), shape((2, slim, columns), F32),
        ),
        in_specs=[far] * 11,
        out_specs=[vmem] * 5,
        scratch_shapes=[
            pltpu.VMEM((tokens, wide), BF16),
            pltpu.VMEM((2, tokens, columns), BF16),
            pltpu.VMEM((tokens, columns), BF16),
            pltpu.VMEM((2, n, rows, rank), BF16),
            pltpu.VMEM((2, rows, columns), F32),
            *[pltpu.VMEM((2, slim, columns), F32)] * 4,
            pltpu.VMEM((tokens, rank), F32),
            pltpu.VMEM((4, 2, depth, slim // 2, columns), F32),
            *[pltpu.VMEM((4, depth, slim // 2, columns), F32)] * 3,
            pltpu.VMEM((2, n, slim, columns), F32),
            pltpu.VMEM((n, slim, columns), F32),
            pltpu.VMEM((tps, 8, columns), F32),
            pltpu.VMEM((3, 2, rows, columns), F32),
            pltpu.VMEM((3, rows, columns), F32),
            dma((11,)),
            *[dma((depth,))] * 4,
            dma((n,)), dma((n,)),
            dma, dma,
            *[dma((2,))] * 6,
            dma((2, n)), dma((2, n)),
            dma((2,)), dma((2,)),
            *[dma((2, 2))] * 4,
            dma((4,)), dma((4,)),
            *[dma((4, depth))] * 6,
            dma((tps,)), dma((tps,)),
            *gather_sems(depth, 4),
        ],
        compiler_params=pltpu.CompilerParams(collective_id=0, has_side_effects=True, vmem_limit_bytes=40 * 2**20),
    )(*[pltpu.with_memory_space_constraint(x, pltpu.HBM) for x in (saved_input, cot_inproj, cot_outproj, factor_inproj, *others)])
    update, fresh, copies, first_new, second_new = results
    copies = copies.reshape(2, n * rows, columns)
    return pl.pallas_call(
        write_kernel,
        out_shape=(
            *[shape((rows, columns), F32)] * 4, *[shape((n * rows, columns), BF16)] * 2, *[shape((slim, columns), F32)] * 4,
        ),
        in_specs=[anywhere] * 5,
        out_specs=[far] * 10,
        scratch_shapes=[dma((10,))],
        compiler_params=pltpu.CompilerParams(vmem_limit_bytes=2**20),
    )(update, fresh, copies, first_new, second_new)


def on_device(saved_input, cot_inproj, cot_outproj, factor_inproj, *others):
    n, tps = lax.axis_size("fs"), lax.axis_size("tp")
    rows, rank = factor_inproj.shape
    if n == 8 and tps == 4 and rank % (16 * n) == 0 and rows % 128 == 0 and cot_inproj.shape[1] % 128 == 0:
        return kernel_form(n, tps, saved_input, cot_inproj, cot_outproj, factor_inproj, *others)
    return plain_form(saved_input, cot_inproj, cot_outproj, factor_inproj, *others)


def solution(mesh):
    return jax.shard_map(
        on_device,
        mesh=mesh,
        in_specs=(
            P("fs", None),
            P("fs", "tp"),
            P("fs", "tp"),
            P("fs", None),
            P("fs", None),
            P("fs", "tp"),
            P("fs", "tp"),
            P("fs", "tp"),
            P("fs", "tp"),
            P("fs", "tp"),
            P("fs", "tp"),
        ),
        out_specs=(
            P("fs", "tp"),
            P("fs", "tp"),
            P("fs", "tp"),
            P("fs", "tp"),
            P(None, "tp"),
            P(None, "tp"),
            P("fs", "tp"),
            P("fs", "tp"),
            P("fs", "tp"),
            P("fs", "tp"),
        ),
        check_vma=False,
    )
```
